32 devices in a mesh: kv: 8 (over z, core), tp: 4 (over y, x).
Axes of the slice: x: 2, y: 2, z: 4, core: 2. Of those that a mesh axis runs over, the one named last changes fastest.
Arguments:
- tokens: bfloat16 [16, 2048], P(None, 'kv'), may hold values from -8 to 8
- lengths: int32 [16], replicated, may hold values from 1 to 3072, 12288 in all
- latent_cache: bfloat16 [16, 3072, 256], P(None, ('kv', 'tp')), may hold values from -10 to 10
- rope_cache: bfloat16 [16, 3072, 32], P(None, ('kv', 'tp')), may hold values from -2000 to 2000
- gain_in: bfloat16 [2048], P('kv'), may hold values from 0.099609375 to 1.8984375
- w_down_q: bfloat16 [2048, 512], P('kv'), may hold values from -0.125 to 0.125
- w_down_kv: bfloat16 [2048, 256], P('kv'), may hold values from -0.125 to 0.125
- w_rope_key: bfloat16 [2048, 32], P('kv'), may hold values from -0.125 to 0.125
- gain_q: bfloat16 [512], replicated, may hold values from 0.099609375 to 1.8984375
- w_up_qn: bfloat16 [512, 16, 64], replicated, may hold values from -0.25 to 0.25
- w_up_qr: bfloat16 [512, 16, 32], replicated, may hold values from -0.25 to 0.25
- gain_kv: bfloat16 [256], replicated, may hold values from 0.099609375 to 1.8984375
- w_key_up: bfloat16 [256, 16, 64], replicated, may hold values from -0.375 to 0.375
- w_value_up: bfloat16 [256, 16, 64], replicated, may hold values from -0.375 to 0.375
- w_attn_out: bfloat16 [16, 64, 2048], P('tp', None, 'kv'), may hold values from -0.1875 to 0.1875
- gain_mid: bfloat16 [2048], P('kv'), may hold values from 0.099609375 to 1.8984375
- w_ff_in: bfloat16 [2048, 8192], P('kv', 'tp'), may hold values from -0.125 to 0.125
- w_ff_out: bfloat16 [8192, 2048], P('tp', 'kv'), may hold values from -0.0625 to 0.0625
Outputs:
- mixed: bfloat16 [16, 2048], P(None, 'kv')
- new_latent: bfloat16 [16, 256], replicated
- new_rope_key: bfloat16 [16, 32], replicated
The draws below stay inside these ranges and needn't reach their ends.
Inputs may be any that keep to these rules, and one draw needn't show every extreme that they name: `lengths`: each sequence's live cache positions; one sequence fills the whole cache.
All inputs are finite; a program needn't handle non-finite values.
Results may differ from the reference program's by a relative error of at most 0.012.
Values sent between devices are 32-bit elements; how exact they have to be, the bound alone decides.
A program may use at most 64 MiB of HBM per device.

```python
import math
import jax
import jax.numpy as jnp
import numpy as np
from jax import lax

D = 2048
H = 16
NOPE = 64
ROPE = 32
V = 64
QR = 512
KR = 256
FF = 8192
SEQS = 16
CACHE = 3072
N_KV = 8


def draw_tokens(key, part):
    first = jax.random.fold_in(key, 0)
    rising = 0.3 * 10.0 ** (jnp.arange(D, dtype=jnp.float32) / D)
    values = jax.random.normal(first, (SEQS, D), jnp.float32) * rising
    return jnp.clip(values, -8.0, 8.0).astype(jnp.bfloat16)


def draw_latent_cache(key, part):
    first = jax.random.fold_in(key, 0)
    values = jax.random.normal(first, (SEQS, CACHE, KR), jnp.float32) * 2.0
    return jnp.clip(values, -10.0, 10.0).astype(jnp.bfloat16)


def draw_rope_cache(key, part):
    first = jax.random.fold_in(key, 0)
    values = jax.random.normal(first, (SEQS, CACHE, ROPE), jnp.float32) * 2.0
    return jnp.clip(values, -2000.0, 2000.0).astype(jnp.bfloat16)


def levels(own_key, dims, cuts, low, top_value):
    factor_of, own = 1.0, jax.random.fold_in(own_key, 6)
    for dim, shards_of in cuts:
        draws = jnp.exp(jax.random.uniform(jax.random.fold_in(own, dim), (shards_of,), jnp.float32, low / len(cuts), top_value / len(cuts)))
        factor_of = factor_of * jnp.repeat(draws, dims[dim] // shards_of).reshape([-1 if axis == dim else 1 for axis in range(len(dims))])
    return factor_of


def profile(count, total, limit, slope):
    portions = [(1 << 20) // math.isqrt(rank ** slope) + 1 for rank in range(2, count + 1)]
    surplus, holding = total - limit - (count - 1), [1] * (count - 1)
    while surplus > 0:
        movable = [i for i in range(count - 1) if holding[i] < limit]
        whole, left = sum([portions[i] for i in movable]), surplus
        for i in movable:
            more = min(limit - holding[i], max(1, left * portions[i] // whole), surplus)
            holding[i] = holding[i] + more
            surplus = surplus - more
    return np.array([limit] + holding)


def uneven(key, amount, total, most, lean):
    if amount == 2:
        one = jax.random.randint(key, (), max(1, total - most), min(most, total - 1) + 1)
        return jnp.stack([one, total - one])
    sizes = jnp.asarray(profile(amount, total, most, lean), jnp.int32)
    pairs = (amount - 1) // 2
    donor, receiver = sizes[1:1 + 2 * pairs:2], sizes[2:2 + 2 * pairs:2]
    slack = jnp.minimum(donor - 1, most - receiver)
    moved = jax.random.randint(jax.random.fold_in(key, 1), (pairs,), 0, 1 << 20) % (slack + 1)
    sizes = sizes.at[1:1 + 2 * pairs:2].set(donor - moved).at[2:2 + 2 * pairs:2].set(receiver + moved)
    return sizes[jax.random.permutation(jax.random.fold_in(key, 2), amount)]


def scatter_about(rng, extent, deviation, most, cuts=(), kind=jnp.bfloat16):
    level = levels(rng, extent, cuts, -0.22, 0.18) if cuts else 1.0
    drawn = jax.random.normal(rng, extent, jnp.float32) * deviation * level
    return jnp.minimum(jnp.maximum(drawn, -most), most).astype(kind)


def setup_inputs(seed: int = 0) -> dict:
    streams_of = jax.random.split(jax.random.key(seed), 19)
    return {
        "tokens": draw_tokens(jax.random.fold_in(streams_of[18], 71), 0),
        "lengths": uneven(streams_of[1], SEQS, SEQS * CACHE // 4, CACHE, 2).astype(jnp.int32),
        "latent_cache": draw_latent_cache(jax.random.fold_in(streams_of[18], 71), 0),
        "rope_cache": draw_rope_cache(jax.random.fold_in(streams_of[18], 71), 0),
        "gain_in": jnp.clip(1.0 + 0.18 * jax.random.normal(streams_of[4], (D,), jnp.float32), 0.099609375, 1.8984375).astype(jnp.bfloat16),
        "w_down_q": scatter_about(streams_of[5], (D, QR), D ** -0.5, 0.125, ((0, 8),)),
        "w_down_kv": scatter_about(streams_of[6], (D, KR), D ** -0.5, 0.125, ((0, 8),)),
        "w_rope_key": scatter_about(streams_of[7], (D, ROPE), D ** -0.5, 0.125, ((0, 8),)),
        "gain_q": jnp.clip(1.0 + 0.18 * jax.random.normal(streams_of[8], (QR,), jnp.float32), 0.099609375, 1.8984375).astype(jnp.bfloat16),
        "w_up_qn": scatter_about(streams_of[9], (QR, H, NOPE), QR ** -0.5, 0.25),
        "w_up_qr": scatter_about(streams_of[10], (QR, H, ROPE), QR ** -0.5, 0.25),
        "gain_kv": jnp.clip(1.0 + 0.18 * jax.random.normal(streams_of[11], (KR,), jnp.float32), 0.099609375, 1.8984375).astype(jnp.bfloat16),
        "w_key_up": scatter_about(streams_of[12], (KR, H, NOPE), KR ** -0.5, 0.375),
        "w_value_up": scatter_about(streams_of[13], (KR, H, V), KR ** -0.5, 0.375),
        "w_attn_out": scatter_about(streams_of[14], (H, V, D), (H * V) ** -0.5, 0.1875, ((0, 4), (2, 8))),
        "gain_mid": jnp.clip(1.0 + 0.18 * jax.random.normal(streams_of[15], (D,), jnp.float32), 0.099609375, 1.8984375).astype(jnp.bfloat16),
        "w_ff_in": scatter_about(streams_of[16], (D, FF), D ** -0.5, 0.125, ((0, 8), (1, 4))),
        "w_ff_out": scatter_about(streams_of[17], (FF, D), FF ** -0.5, 0.0625, ((0, 4), (1, 8))),
    }


EPS = 1e-06

def rotate(values, positions):
    half = values.shape[-1] // 2
    inverse = 10000.0 ** (-jnp.arange(half, dtype=jnp.float32) / half)
    angle = positions.astype(jnp.float32)[:, None, None] * inverse[None, None, :]
    first = values[..., :half]
    second = values[..., half:]
    return jnp.concatenate([first * jnp.cos(angle) - second * jnp.sin(angle), second * jnp.cos(angle) + first * jnp.sin(angle)], axis=-1)

def rms_scaled(values, gain):
    return values * lax.rsqrt(lax.optimization_barrier(jnp.mean(values * values, axis=-1, keepdims=True)) + EPS) * gain.astype(jnp.float32)

def reference(tokens, lengths, latent_cache, rope_cache, gain_in, w_down_q, w_down_kv, w_rope_key, gain_q, w_up_qn, w_up_qr, gain_kv, w_key_up, w_value_up, w_attn_out, gain_mid, w_ff_in, w_ff_out):
    f32 = jnp.float32
    bf16 = jnp.bfloat16
    scale = (NOPE + ROPE) ** (-0.5)
    resid = tokens.astype(f32)
    scaled_in = (resid * gain_in.astype(f32)).astype(bf16)
    inv_in = lax.rsqrt(lax.optimization_barrier(jnp.mean(resid * resid, axis=1, keepdims=True)) + EPS)
    sum_q = jnp.dot(scaled_in, w_down_q, preferred_element_type=f32)
    sum_kv = jnp.dot(scaled_in, w_down_kv, preferred_element_type=f32)
    sum_rope = jnp.dot(scaled_in, w_rope_key, preferred_element_type=f32)
    query_latent = rms_scaled(inv_in * sum_q, gain_q).astype(bf16)
    new_latent = rms_scaled(inv_in * sum_kv, gain_kv).astype(bf16)
    new_rope_key = rotate((inv_in * sum_rope)[:, None, :], lengths)[:, 0, :].astype(bf16)
    query_nope = jnp.einsum('bc,chd->bhd', query_latent.astype(f32), w_up_qn.astype(f32)).astype(bf16)
    query_rope = rotate(jnp.einsum('bc,chr->bhr', query_latent.astype(f32), w_up_qr.astype(f32)), lengths).astype(bf16)
    query_cache = jnp.einsum('bhd,khd->bhk', query_nope.astype(f32), w_key_up.astype(f32)).astype(bf16)
    self_score = (jnp.einsum('bhk,bk->bh', query_cache.astype(f32), new_latent.astype(f32)) + jnp.einsum('bhr,br->bh', query_rope.astype(f32), new_rope_key.astype(f32))) * scale
    span = CACHE // N_KV
    latent_blocks = latent_cache.reshape(SEQS, N_KV, span, KR).swapaxes(0, 1)
    rope_blocks = rope_cache.reshape(SEQS, N_KV, span, ROPE).swapaxes(0, 1)

    def block_scores(args):
        latent_block, rope_block, index = args
        scores = (jnp.einsum('bhk,blk->bhl', query_cache.astype(f32), latent_block.astype(f32)) + jnp.einsum('bhr,blr->bhl', query_rope.astype(f32), rope_block.astype(f32))) * scale
        positions = index * span + jnp.arange(span, dtype=jnp.int32)
        live = positions[None, :] < lengths[:, None]
        return (jnp.where(live[:, None, :], scores, -1e+30), live)
    scores, lives = lax.map(block_scores, (latent_blocks, rope_blocks, jnp.arange(N_KV, dtype=jnp.int32)))
    top = jnp.maximum(lax.optimization_barrier(jnp.max(scores, axis=(0, 3))), self_score)
    weights = jnp.where(lives[:, :, None, :], jnp.exp(scores - top[None, :, :, None]), 0.0)
    self_weight = jnp.exp(self_score - top)
    total = lax.optimization_barrier(jnp.sum(weights, axis=(0, 3))) + self_weight

    def add_block(acc, args):
        weight_block, latent_block = args
        term = jnp.einsum('bhl,blk->bhk', weight_block.astype(bf16).astype(f32), latent_block.astype(f32))
        return (acc + term, None)
    start = self_weight.astype(bf16).astype(f32)[:, :, None] * new_latent.astype(f32)[:, None, :]
    acc, _ = lax.scan(add_block, start, (weights, latent_blocks))
    expanded = jnp.einsum('bhk,khv->bhv', acc, w_value_up.astype(f32), precision=lax.Precision.HIGHEST)
    head_out = (expanded / total[:, :, None]).astype(bf16)
    resid_mid = resid + jnp.einsum('bhv,hvd->bd', head_out.astype(f32), w_attn_out.astype(f32))
    scaled_mid = (resid_mid * gain_mid.astype(f32)).astype(bf16)
    inv_mid = lax.rsqrt(lax.optimization_barrier(jnp.mean(resid_mid * resid_mid, axis=1, keepdims=True)) + EPS)
    hidden = jnp.square(jax.nn.relu(inv_mid * jnp.dot(scaled_mid, w_ff_in, preferred_element_type=f32))).astype(bf16)
    mixed = (resid_mid + jnp.dot(hidden, w_ff_out, preferred_element_type=f32)).astype(bf16)
    return (mixed, new_latent, new_rope_key)
```

```python
import functools

import jax
import jax.numpy as jnp
from jax import lax
from jax.experimental import pallas as pl
from jax.experimental.pallas import tpu as pltpu
from jax.sharding import PartitionSpec as P

D = 2048
NOPE = 64
ROPE = 32


EPS = 1e-06


def combined_all(part, axis, combine):
    gathered = jax.tree.map(lambda a: lax.all_gather(a, axis), part)

    def take(source):
        return jax.tree.map(lambda a: lax.dynamic_index_in_dim(a, source, 0, False), gathered)

    return lax.fori_loop(
        1, lax.axis_size(axis), lambda source, state: combine(state, take(source)), take(0)
    )


def rotate(values, positions):
    half = values.shape[-1] // 2
    inverse = 10000.0 ** (-jnp.arange(half, dtype=jnp.float32) / half)
    angle = positions.astype(jnp.float32)[:, None, None] * inverse[None, None, :]
    first = values[..., :half]
    second = values[..., half:]
    return jnp.concatenate(
        [
            first * jnp.cos(angle) - second * jnp.sin(angle),
            second * jnp.cos(angle) + first * jnp.sin(angle),
        ],
        axis=-1,
    )


def rms_scaled(values, gain):
    return (
        values
        * lax.rsqrt(jnp.mean(values * values, axis=-1, keepdims=True) + EPS)
        * gain.astype(jnp.float32)
    )


def combine(earlier, later):
    top_a, total_a, acc_a = earlier
    top_b, total_b, acc_b = later
    top = jnp.maximum(top_a, top_b)
    fade_a = jnp.exp(top_a - top)
    fade_b = jnp.exp(top_b - top)
    return (
        top,
        total_a * fade_a + total_b * fade_b,
        acc_a * fade_a[..., None] + acc_b * fade_b[..., None],
    )


def fold_sources(parts):
    tops, totals, accs = parts
    top = jnp.max(tops, axis=0)
    fade = jnp.exp(tops - top[None])
    return (top, jnp.sum(totals * fade, axis=0), jnp.sum(accs * fade[..., None], axis=0))


def per_device(
    tokens,
    lengths,
    latent_cache,
    rope_cache,
    gain_in,
    w_down_q,
    w_down_kv,
    w_rope_key,
    gain_q,
    w_up_qn,
    w_up_qr,
    gain_kv,
    w_key_up,
    w_value_up,
    w_attn_out,
    gain_mid,
    w_ff_in,
    w_ff_out,
):
    f32 = jnp.float32
    bf16 = jnp.bfloat16
    highest = lax.Precision.HIGHEST
    scale = (NOPE + ROPE) ** (-0.5)
    resid = tokens.astype(f32)
    scaled_in = (resid * gain_in.astype(f32)).astype(bf16)
    part_q = jnp.dot(scaled_in, w_down_q, preferred_element_type=f32)
    part_kv = jnp.dot(scaled_in, w_down_kv, preferred_element_type=f32)
    part_rope = jnp.dot(scaled_in, w_rope_key, preferred_element_type=f32)
    square_in = jnp.sum(resid * resid, axis=1)
    sum_q, sum_kv, sum_rope, total_in = lax.psum((part_q, part_kv, part_rope, square_in), "kv")
    inv_in = lax.rsqrt(total_in / D + EPS)[:, None]
    query_latent = rms_scaled(inv_in * sum_q, gain_q).astype(bf16)
    new_latent = rms_scaled(inv_in * sum_kv, gain_kv).astype(bf16)
    new_rope_key = rotate((inv_in * sum_rope)[:, None, :], lengths)[:, 0, :].astype(bf16)
    query_nope = jnp.einsum(
        "bc,chd->bhd", query_latent, w_up_qn, preferred_element_type=f32
    ).astype(bf16)
    query_rope = rotate(
        jnp.einsum("bc,chr->bhr", query_latent, w_up_qr, preferred_element_type=f32), lengths
    ).astype(bf16)
    query_cache = jnp.einsum(
        "bhd,khd->bhk", query_nope, w_key_up, preferred_element_type=f32
    ).astype(bf16)
    rows = latent_cache.shape[1]
    positions = lax.axis_index(("kv", "tp")) * rows + jnp.arange(rows, dtype=jnp.int32)
    live = (positions[None, :] < lengths[:, None])[:, None, :]
    scores = (
        jnp.einsum("bhk,blk->bhl", query_cache, latent_cache, preferred_element_type=f32)
        + jnp.einsum("bhr,blr->bhl", query_rope, rope_cache, preferred_element_type=f32)
    ) * scale
    scores = jnp.where(live, scores, -1e30)
    top = jnp.max(scores, axis=2)
    weights = jnp.where(live, jnp.exp(scores - top[:, :, None]), 0.0)
    total = jnp.sum(weights, axis=2)
    acc = jnp.einsum("bhl,blk->bhk", weights.astype(bf16), latent_cache, preferred_element_type=f32)
    heads_dev = w_attn_out.shape[0]
    first_head = lax.axis_index("tp") * heads_dev
    own_value_up = lax.dynamic_slice_in_dim(w_value_up, first_head, heads_dev, 1).astype(f32)
    own_cache_q = lax.dynamic_slice_in_dim(query_cache, first_head, heads_dev, 1)
    own_rope_q = lax.dynamic_slice_in_dim(query_rope, first_head, heads_dev, 1)
    self_score = (
        jnp.einsum("bhk,bk->bh", own_cache_q, new_latent, preferred_element_type=f32)
        + jnp.einsum("bhr,br->bh", own_rope_q, new_rope_key, preferred_element_type=f32)
    ) * scale
    top, total, acc = fold_sources(
        (
            lax.all_to_all(top[None], "tp", split_axis=2, concat_axis=0, tiled=True),
            lax.all_to_all(total[None], "tp", split_axis=2, concat_axis=0, tiled=True),
            lax.all_to_all(acc[None], "tp", split_axis=2, concat_axis=0, tiled=True),
        )
    )
    top, total, acc = combined_all((top, total, acc), "kv", combine)
    joined = jnp.maximum(top, self_score)
    fade = jnp.exp(top - joined)
    self_weight = jnp.exp(self_score - joined)
    total = total * fade + self_weight
    acc = (
        acc * fade[:, :, None]
        + self_weight.astype(bf16).astype(f32)[:, :, None] * new_latent.astype(f32)[:, None, :]
    )
    expanded = jnp.einsum("bhk,khv->bhv", acc, own_value_up, precision=highest)
    head_out = (expanded / total[:, :, None]).astype(bf16)
    attn_part = jnp.einsum("bhv,hvd->bd", head_out, w_attn_out, preferred_element_type=f32)
    resid_mid = resid + lax.psum(attn_part, "tp")
    scaled_mid = (resid_mid * gain_mid.astype(f32)).astype(bf16)
    hidden_part = jnp.dot(scaled_mid, w_ff_in, preferred_element_type=f32)
    square_mid = jnp.sum(resid_mid * resid_mid, axis=1)
    hidden_sum, total_mid = lax.psum((hidden_part, square_mid), "kv")
    inv_mid = lax.rsqrt(total_mid / D + EPS)[:, None]
    hidden = jnp.square(jax.nn.relu(inv_mid * hidden_sum)).astype(bf16)
    out_part = jnp.dot(hidden, w_ff_out, preferred_element_type=f32)
    mixed = (resid_mid + lax.psum(out_part, "tp")).astype(bf16)
    return (mixed, new_latent, new_rope_key)

MESH = pl.DeviceIdType.MESH
LANES = 128


def dot_nt(a, b):
    return lax.dot_general(a, b, (((1,), (1,)), ((), ())), preferred_element_type=jnp.float32)


def dot_nn(a, b):
    return jnp.dot(a, b, preferred_element_type=jnp.float32)


def turn(values, cos, sin, half):
    width = values.shape[1]
    lane = lax.broadcasted_iota(jnp.int32, values.shape, 1)
    partner = jnp.where(
        lane % (2 * half) < half,
        -pltpu.roll(values, width - half, 1),
        pltpu.roll(values, half, 1),
    )
    return values * cos + partner * sin


def layer_kernel(
    n_kv, n_tp,
    tokens, lengths, gain_in, gain_q, gain_kv, gain_mid,
    latent_h, rope_h, down_q_h, down_kv_h, down_r_h, up_qn_h, up_qr_h, key_up_h, value_up_h,
    attn_out_h, ff_in_h, ff_out_h,
    mixed_ref, new_latent_ref, new_rope_ref,
    latent, rope, down_q, down_kv, down_r, up_qn, up_qr, key_up, value_up, attn_out, ff_in, ff_out,
    part_in, got_in, full_in, q_rows, r_rows, acc_rows, part_att, got_att, head_rows,
    part_out, got_out, part_stat, got_stat, part_ff, got_ff, full_ff, part_mix, got_mix,
    load_sem, send_sem, recv_sem,
):
    f32 = jnp.float32
    bf16 = jnp.bfloat16
    kv = lax.axis_index("kv")
    tp = lax.axis_index("tp")
    n_all = n_kv * n_tp
    me = kv * n_tp + tp
    loads = []
    for i, (src, dst) in enumerate((
        (down_q_h, down_q), (down_kv_h, down_kv), (down_r_h, down_r), (up_qn_h, up_qn),
        (up_qr_h, up_qr), (key_up_h, key_up), (latent_h, latent), (rope_h, rope),
        (value_up_h, value_up), (attn_out_h, attn_out), (ff_in_h, ff_in), (ff_out_h, ff_out),
    )):
        copy = pltpu.make_async_copy(src, dst, load_sem.at[i])
        copy.start()
        loads.append(copy)

    barrier = pltpu.get_barrier_semaphore()
    for d in range(1, n_all):
        peer = lax.rem(me + d, n_all)
        pl.semaphore_signal(
            barrier, inc=1, device_id=(peer // n_tp, lax.rem(peer, n_tp)), device_id_type=MESH
        )

    def remote(src, dst, slot, where):
        return pltpu.make_async_remote_copy(
            src_ref=src, dst_ref=dst, send_sem=send_sem.at[slot], recv_sem=recv_sem.at[slot],
            device_id=where, device_id_type=MESH,
        )

    sent = []
    slots = [0]

    def begin(axis, src_of, dst_of):
        count, mine = {"kv": (n_kv, kv), "tp": (n_tp, tp), "all": (n_all, me)}[axis]
        base = slots[0]
        slots[0] += count - 1

        def where(index):
            if axis == "kv":
                return (index, tp)
            if axis == "tp":
                return (kv, index)
            return (index // n_tp, lax.rem(index, n_tp))

        arriving = []
        for d in range(1, count):
            peer = lax.rem(mine + d, count)
            copy = remote(src_of(peer), dst_of(mine), base + d - 1, where(peer))
            copy.start()
            sent.append(copy)
            source = lax.rem(mine + count - d, count)
            arriving.append(remote(dst_of(source), dst_of(source), base + d - 1, where(source)))

        def finish():
            for copy in arriving:
                copy.wait_recv()

        return finish

    seqs, width = tokens.shape
    q_rank = down_q.shape[1]
    kv_rank = down_kv.shape[1]
    rope_size = down_r.shape[0]
    half = rope_size // 2
    heads = key_up.shape[0]
    nope = key_up.shape[1]
    v_size = value_up.shape[1]
    rows = latent.shape[1]
    own_heads = heads // n_tp
    own_seqs = seqs // n_kv
    scale = (nope + rope_size) ** (-0.5)
    d_model = width * n_kv

    resid = tokens[...].astype(f32)
    scaled_in = (resid * gain_in[...].astype(f32)).astype(bf16)
    for copy in loads[:3]:
        copy.wait()
    square = jnp.sum(resid * resid, axis=1, keepdims=True)
    part = jnp.concatenate(
        [
            dot_nn(scaled_in, down_q[...]),
            dot_nn(scaled_in, down_kv[...]),
            dot_nt(scaled_in, down_r[...]),
            jnp.zeros((seqs, LANES - rope_size), f32),
            jnp.broadcast_to(square, (seqs, LANES)),
        ],
        axis=1,
    )
    block = part.shape[1] // n_tp
    for i in range(n_tp):
        part_in[i] = part[:, i * block : (i + 1) * block]
    pl.semaphore_wait(barrier, n_all - 1)
    finish = begin("kv", lambda k: part_in.at[tp], lambda k: got_in.at[k])
    got_in[kv] = part_in[tp]

    lane = lax.broadcasted_iota(jnp.int32, (seqs, LANES), 1)
    row = lax.broadcasted_iota(jnp.int32, (seqs, LANES), 0)
    where_at = jnp.zeros((seqs, LANES), jnp.int32)
    for b in range(seqs):
        where_at = jnp.where(row == b, lengths[b], where_at)
    inverse = jnp.zeros((seqs, LANES), f32)
    for j in range(half):
        inverse = jnp.where(lane % half == j, 10000.0 ** (-j / half), inverse)
    angle = where_at.astype(f32) * inverse
    cos, sin = jnp.cos(angle), jnp.sin(angle)
    finish()
    full_in[tp] = jnp.sum(got_in[...], axis=0)
    finish = begin("tp", lambda t: full_in.at[tp], lambda t: full_in.at[t])
    for copy in loads[3:6]:
        copy.wait()
    finish()
    sums = jnp.concatenate([full_in[i] for i in range(n_tp)], axis=1)
    inv_in = lax.rsqrt(sums[:, q_rank + kv_rank + LANES :][:, :1] / d_model + EPS)
    lat_q = inv_in * sums[:, :q_rank]
    query_latent = (
        lat_q
        * lax.rsqrt(jnp.mean(lat_q * lat_q, axis=1, keepdims=True) + EPS)
        * gain_q[...].astype(f32)
    ).astype(bf16)
    lat_kv = inv_in * sums[:, q_rank : q_rank + kv_rank]
    new_latent = (
        lat_kv
        * lax.rsqrt(jnp.mean(lat_kv * lat_kv, axis=1, keepdims=True) + EPS)
        * gain_kv[...].astype(f32)
    ).astype(bf16)
    new_latent_ref[...] = new_latent
    new_latent = new_latent.astype(f32)
    new_rope = turn(
        inv_in * sums[:, q_rank + kv_rank : q_rank + kv_rank + LANES], cos, sin, half
    ).astype(bf16)
    new_rope_ref[...] = new_rope[:, :rope_size]
    new_rope = new_rope.astype(f32)[:, :rope_size]

    query_nope = dot_nt(query_latent, up_qn[...]).astype(bf16)
    times = heads * rope_size // LANES
    query_rope = turn(
        dot_nt(query_latent, up_qr[...]),
        jnp.concatenate([cos] * times, axis=1),
        jnp.concatenate([sin] * times, axis=1),
        half,
    ).astype(bf16).astype(f32)
    for h in range(heads):
        q_rows[h] = dot_nn(query_nope[:, h * nope : (h + 1) * nope], key_up[h]).astype(
            bf16
        ).astype(f32)
        r_rows[h] = query_rope[:, h * rope_size : (h + 1) * rope_size]

    for copy in loads[6:9]:
        copy.wait()
    first = me * rows
    at = first + lax.broadcasted_iota(jnp.int32, (heads, rows), 1)
    scores, selfs, lives = [], [], []
    for b in range(seqs):
        q_b = q_rows[:, b, :]
        r_b = r_rows[:, b, :]
        score = (
            dot_nt(q_b.astype(bf16), latent[b]) + dot_nn(r_b.astype(bf16), rope[b])
        ) * scale
        live = at < lengths[b]
        scores.append(jnp.where(live, score, -1e30))
        lives.append(live)
        own = (
            jnp.sum(q_b * new_latent[b : b + 1, :], axis=1, keepdims=True)
            + jnp.sum(r_b * new_rope[b : b + 1, :], axis=1, keepdims=True)
        ) * scale
        selfs.append(own)
    mine = me == 0
    for b in range(seqs):
        own = jnp.where(mine, selfs[b], -1e30)
        top = jnp.maximum(jnp.max(scores[b], axis=1, keepdims=True), own)
        weights = jnp.where(lives[b], jnp.exp(scores[b] - top), 0.0)
        own_weight = jnp.where(mine, jnp.exp(own - top), 0.0)
        total = jnp.sum(weights, axis=1, keepdims=True) + own_weight
        acc_rows[b, :, :kv_rank] = (
            dot_nn(weights.astype(bf16), latent[b])
            + own_weight.astype(bf16).astype(f32) * new_latent[b : b + 1, :]
        )
        acc_rows[b, :, kv_rank : kv_rank + LANES] = jnp.broadcast_to(top, (heads, LANES))
        acc_rows[b, :, kv_rank + LANES :] = jnp.broadcast_to(total, (heads, LANES))

    v_wide = own_heads * v_size
    for t in range(n_tp):
        pieces = []
        stat = jnp.zeros((seqs, LANES), f32)
        for i in range(own_heads):
            h = t * own_heads + i
            acc = acc_rows[:, h, :]
            exact = acc[:, :kv_rank]
            high = exact.astype(bf16)
            low = (exact - high.astype(f32)).astype(bf16)
            both = dot_nt(jnp.concatenate([high, low], axis=0), value_up[h])
            pieces.append(both[:seqs] + both[seqs:])
            stat = jnp.where(lane == i, acc[:, kv_rank : kv_rank + LANES], stat)
            stat = jnp.where(lane == own_heads + i, acc[:, kv_rank + LANES :], stat)
        message = jnp.concatenate(pieces + [stat], axis=1)
        for k in range(n_kv):
            part_att[k * n_tp + t] = message[k * own_seqs : (k + 1) * own_seqs, :]
    finish = begin("all", lambda p: part_att.at[p], lambda p: got_att.at[p])
    got_att[me] = part_att[me]
    finish()
    got = got_att[...]
    values = got[:, :, :v_wide]
    stat = got[:, :, v_wide:]
    fade_all = jnp.exp(stat - jnp.max(stat, axis=0, keepdims=True))
    head_lane = lax.broadcasted_iota(jnp.int32, values.shape, 2) // v_size
    sum_lane = lax.broadcasted_iota(jnp.int32, (own_seqs, v_wide), 1) // v_size
    fade = jnp.zeros(values.shape, f32)
    total = jnp.ones((own_seqs, v_wide), f32)
    for i in range(own_heads):
        fade_i = fade_all[:, :, i : i + 1]
        total_i = jnp.sum(stat[:, :, own_heads + i : own_heads + i + 1] * fade_i, axis=0)
        fade = jnp.where(head_lane == i, fade_i, fade)
        total = jnp.where(sum_lane == i, total_i, total)
    head_rows[kv] = (jnp.sum(values * fade, axis=0) / total).astype(bf16).astype(f32)
    finish = begin("kv", lambda k: head_rows.at[kv], lambda k: head_rows.at[k])
    loads[9].wait()
    finish()
    head_out = jnp.concatenate([head_rows[k] for k in range(n_kv)], axis=0).astype(bf16)

    got_out[tp] = dot_nn(head_out, attn_out[...])
    finish = begin("tp", lambda t: got_out.at[tp], lambda t: got_out.at[t])
    loads[10].wait()
    finish()
    resid_mid = resid + jnp.sum(got_out[...], axis=0)
    got_stat[kv] = jnp.broadcast_to(
        jnp.sum(resid_mid * resid_mid, axis=1, keepdims=True), (seqs, LANES)
    )
    finish_stat = begin("kv", lambda k: got_stat.at[kv], lambda k: got_stat.at[k])
    scaled_mid = (resid_mid * gain_mid[...].astype(f32)).astype(bf16)
    hidden_part = dot_nn(scaled_mid, ff_in[...])
    piece = hidden_part.shape[1] // n_kv
    for k in range(n_kv):
        part_ff[k] = hidden_part[:, k * piece : (k + 1) * piece]
    finish = begin("kv", lambda k: part_ff.at[k], lambda k: got_ff.at[k])
    got_ff[kv] = part_ff[kv]
    finish_stat()
    inv_mid = lax.rsqrt(jnp.sum(got_stat[...], axis=0)[:, :1] / d_model + EPS)
    loads[11].wait()
    finish()
    full_ff[kv] = jnp.sum(got_ff[...], axis=0)
    finish = begin("kv", lambda k: full_ff.at[kv], lambda k: full_ff.at[k])
    finish()
    hidden_sum = jnp.concatenate([full_ff[k] for k in range(n_kv)], axis=1)
    hidden = jnp.square(jnp.maximum(inv_mid * hidden_sum, 0.0)).astype(bf16)
    got_mix[tp] = dot_nn(hidden, ff_out[...])
    finish = begin("tp", lambda t: got_mix.at[tp], lambda t: got_mix.at[t])
    finish()
    mixed_ref[...] = (resid_mid + jnp.sum(got_mix[...], axis=0)).astype(bf16)
    for copy in sent:
        copy.wait_send()


def per_device_kernel(
    n_kv, n_tp,
    tokens, lengths, latent_cache, rope_cache, gain_in, w_down_q, w_down_kv, w_rope_key, gain_q,
    w_up_qn, w_up_qr, gain_kv, w_key_up, w_value_up, w_attn_out, gain_mid, w_ff_in, w_ff_out,
):
    f32 = jnp.float32
    bf16 = jnp.bfloat16
    seqs, width = tokens.shape
    q_rank, heads, nope = w_up_qn.shape
    kv_rank, _, v_size = w_value_up.shape
    rope_size = w_rope_key.shape[1]
    hidden = w_ff_in.shape[1]
    n_all = n_kv * n_tp
    own_seqs = seqs // n_kv
    v_wide = heads // n_tp * v_size
    big = [
        latent_cache,
        rope_cache.transpose(0, 2, 1),
        w_down_q,
        w_down_kv,
        w_rope_key.T,
        w_up_qn.transpose(1, 2, 0).reshape(heads * nope, q_rank),
        w_up_qr.transpose(1, 2, 0).reshape(heads * rope_size, q_rank),
        w_key_up.transpose(1, 2, 0),
        w_value_up.transpose(1, 2, 0),
        w_attn_out.reshape(-1, width),
        w_ff_in,
        w_ff_out,
    ]
    block = (q_rank + kv_rank + 2 * LANES) // n_tp
    messages = 5 * (n_kv - 1) + 3 * (n_tp - 1) + (n_all - 1)
    vmem = pltpu.VMEM
    whole = pl.BlockSpec(memory_space=pltpu.VMEM)
    return pl.pallas_call(
        functools.partial(layer_kernel, n_kv, n_tp),
        out_shape=(
            jax.ShapeDtypeStruct((seqs, width), bf16),
            jax.ShapeDtypeStruct((seqs, kv_rank), bf16),
            jax.ShapeDtypeStruct((seqs, rope_size), bf16),
        ),
        in_specs=[whole, pl.BlockSpec(memory_space=pltpu.SMEM)]
        + [whole] * 4
        + [pl.BlockSpec(memory_space=pl.ANY)] * len(big),
        out_specs=(whole, whole, whole),
        scratch_shapes=[vmem(a.shape, bf16) for a in big]
        + [
            vmem((n_tp, seqs, block), f32),
            vmem((n_kv, seqs, block), f32),
            vmem((n_tp, seqs, block), f32),
            vmem((heads, seqs, kv_rank), f32),
            vmem((heads, seqs, rope_size), f32),
            vmem((seqs, heads, kv_rank + 2 * LANES), f32),
            vmem((n_all, own_seqs, v_wide + LANES), f32),
            vmem((n_all, own_seqs, v_wide + LANES), f32),
            vmem((n_kv, own_seqs, v_wide), f32),
            vmem((8, LANES), f32),
            vmem((n_tp, seqs, width), f32),
            vmem((8, LANES), f32),
            vmem((n_kv, seqs, LANES), f32),
            vmem((n_kv, seqs, hidden // n_kv), f32),
            vmem((n_kv, seqs, hidden // n_kv), f32),
            vmem((n_kv, seqs, hidden // n_kv), f32),
            vmem((8, LANES), f32),
            vmem((n_tp, seqs, width), f32),
            pltpu.SemaphoreType.DMA((len(big),)),
            pltpu.SemaphoreType.DMA((messages,)),
            pltpu.SemaphoreType.DMA((messages,)),
        ],
        compiler_params=pltpu.CompilerParams(collective_id=0, has_side_effects=True),
        name="layer",
    )(
        tokens, lengths, gain_in.reshape(1, -1), gain_q.reshape(1, -1), gain_kv.reshape(1, -1),
        gain_mid.reshape(1, -1), *big,
    )


def kernel_fits(n_kv, n_tp, seqs, width, q_rank, kv_rank, rope_size, heads, v_size, hidden):
    return (
        seqs % n_kv == 0
        and heads % n_tp == 0
        and width % LANES == 0
        and q_rank % LANES == 0
        and kv_rank % LANES == 0
        and LANES % rope_size == 0
        and (heads * rope_size) % LANES == 0
        and (q_rank + kv_rank + 2 * LANES) % (n_tp * LANES) == 0
        and (heads // n_tp * v_size) % LANES == 0
        and hidden % (n_kv * LANES) == 0
    )


def per_device_any(n_kv, n_tp, *args):
    tokens, w_down_q, w_down_kv, w_rope_key = args[0], args[5], args[6], args[7]
    w_value_up, w_ff_in = args[13], args[16]
    if kernel_fits(
        n_kv, n_tp, *tokens.shape, w_down_q.shape[1], w_down_kv.shape[1], w_rope_key.shape[1],
        *w_value_up.shape[1:], w_ff_in.shape[1],
    ):
        return per_device_kernel(n_kv, n_tp, *args)
    return per_device(*args)


def solution(mesh):
    return jax.shard_map(
        functools.partial(per_device_any, mesh.shape["kv"], mesh.shape["tp"]),
        mesh=mesh,
        in_specs=(
            P(None, "kv"),
            P(),
            P(None, ("kv", "tp"), None),
            P(None, ("kv", "tp"), None),
            P("kv"),
            P("kv", None),
            P("kv", None),
            P("kv", None),
            P(),
            P(),
            P(),
            P(),
            P(),
            P(),
            P("tp", None, "kv"),
            P("kv"),
            P("kv", "tp"),
            P("tp", "kv"),
        ),
        out_specs=(P(None, "kv"), P(), P()),
        check_vma=False,
    )
```

```python
import functools

import jax
import jax.numpy as jnp
from jax import lax
from jax.experimental import pallas as pl
from jax.experimental.pallas import tpu as pltpu
from jax.sharding import PartitionSpec as P

D = 2048
NOPE = 64
ROPE = 32


EPS = 1e-06


def combined_all(part, axis, combine):
    gathered = jax.tree.map(lambda a: lax.all_gather(a, axis), part)

    def take(source):
        return jax.tree.map(lambda a: lax.dynamic_index_in_dim(a, source, 0, False), gathered)

    return lax.fori_loop(
        1, lax.axis_size(axis), lambda source, state: combine(state, take(source)), take(0)
    )


def rotate(values, positions):
    half = values.shape[-1] // 2
    inverse = 10000.0 ** (-jnp.arange(half, dtype=jnp.float32) / half)
    angle = positions.astype(jnp.float32)[:, None, None] * inverse[None, None, :]
    first = values[..., :half]
    second = values[..., half:]
    return jnp.concatenate(
        [
            first * jnp.cos(angle) - second * jnp.sin(angle),
            second * jnp.cos(angle) + first * jnp.sin(angle),
        ],
        axis=-1,
    )


def rms_scaled(values, gain):
    return (
        values
        * lax.rsqrt(jnp.mean(values * values, axis=-1, keepdims=True) + EPS)
        * gain.astype(jnp.float32)
    )


def combine(earlier, later):
    top_a, total_a, acc_a = earlier
    top_b, total_b, acc_b = later
    top = jnp.maximum(top_a, top_b)
    fade_a = jnp.exp(top_a - top)
    fade_b = jnp.exp(top_b - top)
    return (
        top,
        total_a * fade_a + total_b * fade_b,
        acc_a * fade_a[..., None] + acc_b * fade_b[..., None],
    )


def fold_sources(parts):
    tops, totals, accs = parts
    top = jnp.max(tops, axis=0)
    fade = jnp.exp(tops - top[None])
    return (top, jnp.sum(totals * fade, axis=0), jnp.sum(accs * fade[..., None], axis=0))


def per_device(
    tokens,
    lengths,
    latent_cache,
    rope_cache,
    gain_in,
    w_down_q,
    w_down_kv,
    w_rope_key,
    gain_q,
    w_up_qn,
    w_up_qr,
    gain_kv,
    w_key_up,
    w_value_up,
    w_attn_out,
    gain_mid,
    w_ff_in,
    w_ff_out,
):
    f32 = jnp.float32
    bf16 = jnp.bfloat16
    highest = lax.Precision.HIGHEST
    scale = (NOPE + ROPE) ** (-0.5)
    resid = tokens.astype(f32)
    scaled_in = (resid * gain_in.astype(f32)).astype(bf16)
    part_q = jnp.dot(scaled_in, w_down_q, preferred_element_type=f32)
    part_kv = jnp.dot(scaled_in, w_down_kv, preferred_element_type=f32)
    part_rope = jnp.dot(scaled_in, w_rope_key, preferred_element_type=f32)
    square_in = jnp.sum(resid * resid, axis=1)
    sum_q, sum_kv, sum_rope, total_in = lax.psum((part_q, part_kv, part_rope, square_in), "kv")
    inv_in = lax.rsqrt(total_in / D + EPS)[:, None]
    query_latent = rms_scaled(inv_in * sum_q, gain_q).astype(bf16)
    new_latent = rms_scaled(inv_in * sum_kv, gain_kv).astype(bf16)
    new_rope_key = rotate((inv_in * sum_rope)[:, None, :], lengths)[:, 0, :].astype(bf16)
    query_nope = jnp.einsum(
        "bc,chd->bhd", query_latent, w_up_qn, preferred_element_type=f32
    ).astype(bf16)
    query_rope = rotate(
        jnp.einsum("bc,chr->bhr", query_latent, w_up_qr, preferred_element_type=f32), lengths
    ).astype(bf16)
    query_cache = jnp.einsum(
        "bhd,khd->bhk", query_nope, w_key_up, preferred_element_type=f32
    ).astype(bf16)
    rows = latent_cache.shape[1]
    positions = lax.axis_index(("kv", "tp")) * rows + jnp.arange(rows, dtype=jnp.int32)
    live = (positions[None, :] < lengths[:, None])[:, None, :]
    scores = (
        jnp.einsum("bhk,blk->bhl", query_cache, latent_cache, preferred_element_type=f32)
        + jnp.einsum("bhr,blr->bhl", query_rope, rope_cache, preferred_element_type=f32)
    ) * scale
    scores = jnp.where(live, scores, -1e30)
    top = jnp.max(scores, axis=2)
    weights = jnp.where(live, jnp.exp(scores - top[:, :, None]), 0.0)
    total = jnp.sum(weights, axis=2)
    acc = jnp.einsum("bhl,blk->bhk", weights.astype(bf16), latent_cache, preferred_element_type=f32)
    heads_dev = w_attn_out.shape[0]
    first_head = lax.axis_index("tp") * heads_dev
    own_value_up = lax.dynamic_slice_in_dim(w_value_up, first_head, heads_dev, 1).astype(f32)
    own_cache_q = lax.dynamic_slice_in_dim(query_cache, first_head, heads_dev, 1)
    own_rope_q = lax.dynamic_slice_in_dim(query_rope, first_head, heads_dev, 1)
    self_score = (
        jnp.einsum("bhk,bk->bh", own_cache_q, new_latent, preferred_element_type=f32)
        + jnp.einsum("bhr,br->bh", own_rope_q, new_rope_key, preferred_element_type=f32)
    ) * scale
    top, total, acc = fold_sources(
        (
            lax.all_to_all(top[None], "tp", split_axis=2, concat_axis=0, tiled=True),
            lax.all_to_all(total[None], "tp", split_axis=2, concat_axis=0, tiled=True),
            lax.all_to_all(acc[None], "tp", split_axis=2, concat_axis=0, tiled=True),
        )
    )
    top, total, acc = combined_all((top, total, acc), "kv", combine)
    joined = jnp.maximum(top, self_score)
    fade = jnp.exp(top - joined)
    self_weight = jnp.exp(self_score - joined)
    total = total * fade + self_weight
    acc = (
        acc * fade[:, :, None]
        + self_weight.astype(bf16).astype(f32)[:, :, None] * new_latent.astype(f32)[:, None, :]
    )
    expanded = jnp.einsum("bhk,khv->bhv", acc, own_value_up, precision=highest)
    head_out = (expanded / total[:, :, None]).astype(bf16)
    attn_part = jnp.einsum("bhv,hvd->bd", head_out, w_attn_out, preferred_element_type=f32)
    resid_mid = resid + lax.psum(attn_part, "tp")
    scaled_mid = (resid_mid * gain_mid.astype(f32)).astype(bf16)
    hidden_part = jnp.dot(scaled_mid, w_ff_in, preferred_element_type=f32)
    square_mid = jnp.sum(resid_mid * resid_mid, axis=1)
    hidden_sum, total_mid = lax.psum((hidden_part, square_mid), "kv")
    inv_mid = lax.rsqrt(total_mid / D + EPS)[:, None]
    hidden = jnp.square(jax.nn.relu(inv_mid * hidden_sum)).astype(bf16)
    out_part = jnp.dot(hidden, w_ff_out, preferred_element_type=f32)
    mixed = (resid_mid + lax.psum(out_part, "tp")).astype(bf16)
    return (mixed, new_latent, new_rope_key)

MESH = pl.DeviceIdType.MESH
LANES = 128


def dot_nt(a, b):
    return lax.dot_general(a, b, (((1,), (1,)), ((), ())), preferred_element_type=jnp.float32)


def dot_nn(a, b):
    return jnp.dot(a, b, preferred_element_type=jnp.float32)


def turn(values, cos, sin, half):
    width = values.shape[1]
    lane = lax.broadcasted_iota(jnp.int32, values.shape, 1)
    partner = jnp.where(
        lane % (2 * half) < half,
        -pltpu.roll(values, width - half, 1),
        pltpu.roll(values, half, 1),
    )
    return values * cos + partner * sin


def layer_kernel(
    n_kv, n_tp,
    tokens_h, gain_in_h, lengths_h, gain_q_h, gain_kv_h, gain_mid_h,
    latent_h, rope_h, down_q_h, down_kv_h, down_r_h, up_qn_h, up_qr_h, key_up_h, value_up_h,
    attn_out_h, ff_in_h, ff_out_h,
    mixed_ref, new_latent_ref, new_rope_ref,
    tokens, gain_in, lengths, gain_q, gain_kv, gain_mid,
    latent, rope, down_q, down_kv, down_r, up_qn, up_qr, key_up, value_up, attn_out, ff_in, ff_out,
    part_in, got_in, full_in, q_rows, r_rows, acc_rows, part_att, got_att, part_seq, got_seq,
    head_rows, got_out, got_stat, part_ff, got_ff, full_ff, got_mix,
    load_sem, send_sem, recv_sem,
):
    f32 = jnp.float32
    bf16 = jnp.bfloat16
    kv = lax.axis_index("kv")
    tp = lax.axis_index("tp")
    me = kv * n_tp + tp
    loads = [
        pltpu.make_async_copy(src, dst, load_sem.at[i])
        for i, (src, dst) in enumerate((
            (tokens_h, tokens), (gain_in_h, gain_in), (down_q_h, down_q), (down_kv_h, down_kv),
            (down_r_h, down_r), (lengths_h, lengths), (gain_q_h, gain_q), (gain_kv_h, gain_kv),
            (gain_mid_h, gain_mid), (up_qn_h, up_qn), (up_qr_h, up_qr), (key_up_h, key_up),
            (latent_h, latent), (rope_h, rope), (value_up_h, value_up), (attn_out_h, attn_out),
            (ff_in_h, ff_in), (ff_out_h, ff_out),
        ))
    ]
    for copy in loads[:9]:
        copy.start()

    barrier = pltpu.get_barrier_semaphore()
    peers = [(lax.rem(kv + d, n_kv), tp) for d in range(1, n_kv)]
    peers += [(kv, lax.rem(tp + d, n_tp)) for d in range(1, n_tp)]
    for peer in peers:
        pl.semaphore_signal(barrier, inc=1, device_id=peer, device_id_type=MESH)

    def remote(src, dst, slot, where):
        return pltpu.make_async_remote_copy(
            src_ref=src, dst_ref=dst, send_sem=send_sem.at[slot], recv_sem=recv_sem.at[slot],
            device_id=where, device_id_type=MESH,
        )

    sent = []
    slots = [0]

    def begin(axis, src_of, dst_of):
        count, mine = {"kv": (n_kv, kv), "tp": (n_tp, tp)}[axis]
        base = slots[0]
        slots[0] += count - 1

        def where(index):
            return (index, tp) if axis == "kv" else (kv, index)

        arriving = []
        for d in range(1, count):
            peer = lax.rem(mine + d, count)
            copy = remote(src_of(peer), dst_of(mine), base + d - 1, where(peer))
            copy.start()
            sent.append(copy)
            source = lax.rem(mine + count - d, count)
            arriving.append(remote(dst_of(source), dst_of(source), base + d - 1, where(source)))

        def finish():
            for copy in arriving:
                copy.wait_recv()

        return finish

    seqs, width = tokens.shape
    q_rank = down_q.shape[1]
    kv_rank = down_kv.shape[1]
    rope_size = down_r.shape[0]
    half = rope_size // 2
    heads = key_up.shape[0]
    nope = key_up.shape[1]
    v_size = value_up.shape[1]
    rows = latent.shape[1]
    own_heads = heads // n_tp
    own_seqs = seqs // n_kv
    scale = (nope + rope_size) ** (-0.5)
    d_model = width * n_kv

    def wide(gain):
        return gain[...].astype(f32)[None, :]

    for copy in loads[:5]:
        copy.wait()
    for copy in loads[9:]:
        copy.start()
    resid = tokens[...].astype(f32)
    scaled_in = (resid * wide(gain_in)).astype(bf16)
    square = jnp.sum(resid * resid, axis=1, keepdims=True)
    part = jnp.concatenate(
        [
            dot_nn(scaled_in, down_q[...]),
            dot_nn(scaled_in, down_kv[...]),
            dot_nt(scaled_in, down_r[...]),
            jnp.zeros((seqs, LANES - rope_size), f32),
            jnp.broadcast_to(square, (seqs, LANES)),
        ],
        axis=1,
    )
    block = part.shape[1] // n_tp
    for i in range(n_tp):
        part_in[i] = part[:, i * block : (i + 1) * block]
    pl.semaphore_wait(barrier, len(peers))
    finish = begin("kv", lambda k: part_in.at[tp], lambda k: got_in.at[k])
    got_in[kv] = part_in[tp]

    for copy in loads[5:9]:
        copy.wait()
    lane = lax.broadcasted_iota(jnp.int32, (seqs, LANES), 1)
    row = lax.broadcasted_iota(jnp.int32, (seqs, LANES), 0)
    where_at = jnp.zeros((seqs, LANES), jnp.int32)
    for b in range(seqs):
        where_at = jnp.where(row == b, lengths[b], where_at)
    inverse = jnp.zeros((seqs, LANES), f32)
    for j in range(half):
        inverse = jnp.where(lane % half == j, 10000.0 ** (-j / half), inverse)
    angle = where_at.astype(f32) * inverse
    cos, sin = jnp.cos(angle), jnp.sin(angle)
    finish()
    full_in[tp] = jnp.sum(got_in[...], axis=0)
    finish = begin("tp", lambda t: full_in.at[tp], lambda t: full_in.at[t])
    for copy in loads[9:12]:
        copy.wait()
    finish()
    sums = jnp.concatenate([full_in[i] for i in range(n_tp)], axis=1)
    inv_in = lax.rsqrt(sums[:, q_rank + kv_rank + LANES :][:, :1] / d_model + EPS)
    lat_q = inv_in * sums[:, :q_rank]
    query_latent = (
        lat_q
        * lax.rsqrt(jnp.mean(lat_q * lat_q, axis=1, keepdims=True) + EPS)
        * wide(gain_q)
    ).astype(bf16)
    lat_kv = inv_in * sums[:, q_rank : q_rank + kv_rank]
    new_latent = (
        lat_kv
        * lax.rsqrt(jnp.mean(lat_kv * lat_kv, axis=1, keepdims=True) + EPS)
        * wide(gain_kv)
    ).astype(bf16)
    new_latent_ref[...] = new_latent
    new_latent = new_latent.astype(f32)
    new_rope = turn(
        inv_in * sums[:, q_rank + kv_rank : q_rank + kv_rank + LANES], cos, sin, half
    ).astype(bf16)
    new_rope_ref[...] = new_rope[:, :rope_size]
    new_rope = new_rope.astype(f32)[:, :rope_size]

    query_nope = dot_nt(query_latent, up_qn[...]).astype(bf16)
    times = heads * rope_size // LANES
    query_rope = turn(
        dot_nt(query_latent, up_qr[...]),
        jnp.concatenate([cos] * times, axis=1),
        jnp.concatenate([sin] * times, axis=1),
        half,
    ).astype(bf16).astype(f32)
    for h in range(heads):
        q_rows[h] = dot_nn(query_nope[:, h * nope : (h + 1) * nope], key_up[h]).astype(
            bf16
        ).astype(f32)
        r_rows[h] = query_rope[:, h * rope_size : (h + 1) * rope_size]

    for copy in loads[12:15]:
        copy.wait()
    first = me * rows
    at = first + lax.broadcasted_iota(jnp.int32, (heads, rows), 1)
    scores, selfs, lives = [], [], []
    for b in range(seqs):
        q_b = q_rows[:, b, :]
        r_b = r_rows[:, b, :]
        score = (
            dot_nt(q_b.astype(bf16), latent[b]) + dot_nn(r_b.astype(bf16), rope[b])
        ) * scale
        live = at < lengths[b]
        scores.append(jnp.where(live, score, -1e30))
        lives.append(live)
        own = (
            jnp.sum(q_b * new_latent[b : b + 1, :], axis=1, keepdims=True)
            + jnp.sum(r_b * new_rope[b : b + 1, :], axis=1, keepdims=True)
        ) * scale
        selfs.append(own)
    mine = me == 0
    for b in range(seqs):
        own = jnp.where(mine, selfs[b], -1e30)
        top = jnp.maximum(jnp.max(scores[b], axis=1, keepdims=True), own)
        weights = jnp.where(lives[b], jnp.exp(scores[b] - top), 0.0)
        own_weight = jnp.where(mine, jnp.exp(own - top), 0.0)
        total = jnp.sum(weights, axis=1, keepdims=True) + own_weight
        acc_rows[b, :, :kv_rank] = (
            dot_nn(weights.astype(bf16), latent[b])
            + own_weight.astype(bf16).astype(f32) * new_latent[b : b + 1, :]
        )
        acc_rows[b, :, kv_rank : kv_rank + LANES] = jnp.broadcast_to(top, (heads, LANES))
        acc_rows[b, :, kv_rank + LANES :] = jnp.broadcast_to(total, (heads, LANES))

    v_wide = own_heads * v_size
    for t in range(n_tp):
        pieces = []
        stat = jnp.zeros((seqs, LANES), f32)
        for i in range(own_heads):
            h = t * own_heads + i
            acc = acc_rows[:, h, :]
            exact = acc[:, :kv_rank]
            high = exact.astype(bf16)
            low = (exact - high.astype(f32)).astype(bf16)
            both = dot_nt(jnp.concatenate([high, low], axis=0), value_up[h])
            pieces.append(both[:seqs] + both[seqs:])
            stat = jnp.where(lane == i, acc[:, kv_rank : kv_rank + LANES], stat)
            stat = jnp.where(lane == own_heads + i, acc[:, kv_rank + LANES :], stat)
        part_att[t] = jnp.concatenate(pieces + [stat], axis=1)
    finish = begin("tp", lambda t: part_att.at[t], lambda t: got_att.at[t])
    got_att[tp] = part_att[tp]
    finish()

    stats = [got_att[t][:, v_wide:] for t in range(n_tp)]
    top = functools.reduce(jnp.maximum, stats)
    head_lane = lax.broadcasted_iota(jnp.int32, (seqs, v_wide), 1) // v_size
    joined = jnp.zeros((seqs, v_wide), f32)
    totals = jnp.zeros((seqs, LANES), f32)
    for t in range(n_tp):
        fade_t = jnp.exp(stats[t] - top)
        fade = jnp.zeros((seqs, v_wide), f32)
        for i in range(own_heads):
            fade = jnp.where(head_lane == i, fade_t[:, i : i + 1], fade)
        joined += got_att[t][:, :v_wide] * fade
        totals += stats[t] * pltpu.roll(fade_t, own_heads, 1)
    message = jnp.concatenate([joined, jnp.where(lane < own_heads, top, totals)], axis=1)
    for k in range(n_kv):
        part_seq[k] = message[k * own_seqs : (k + 1) * own_seqs, :]
    finish = begin("kv", lambda k: part_seq.at[k], lambda k: got_seq.at[k])
    got_seq[kv] = part_seq[kv]
    finish()
    got = got_seq[...]
    values = got[:, :, :v_wide]
    stat = got[:, :, v_wide:]
    fade_all = jnp.exp(stat - jnp.max(stat, axis=0, keepdims=True))
    head_lane = lax.broadcasted_iota(jnp.int32, values.shape, 2) // v_size
    sum_lane = lax.broadcasted_iota(jnp.int32, (own_seqs, v_wide), 1) // v_size
    fade = jnp.zeros(values.shape, f32)
    total = jnp.ones((own_seqs, v_wide), f32)
    for i in range(own_heads):
        fade_i = fade_all[:, :, i : i + 1]
        total_i = jnp.sum(stat[:, :, own_heads + i : own_heads + i + 1] * fade_i, axis=0)
        fade = jnp.where(head_lane == i, fade_i, fade)
        total = jnp.where(sum_lane == i, total_i, total)
    head_rows[kv] = (jnp.sum(values * fade, axis=0) / total).astype(bf16).astype(f32)
    finish = begin("kv", lambda k: head_rows.at[kv], lambda k: head_rows.at[k])
    loads[15].wait()
    finish()
    head_out = jnp.concatenate([head_rows[k] for k in range(n_kv)], axis=0).astype(bf16)

    got_out[tp] = dot_nn(head_out, attn_out[...])
    finish = begin("tp", lambda t: got_out.at[tp], lambda t: got_out.at[t])
    loads[16].wait()
    finish()
    resid_mid = resid + jnp.sum(got_out[...], axis=0)
    got_stat[kv] = jnp.broadcast_to(
        jnp.sum(resid_mid * resid_mid, axis=1, keepdims=True), (seqs, LANES)
    )
    finish_stat = begin("kv", lambda k: got_stat.at[kv], lambda k: got_stat.at[k])
    scaled_mid = (resid_mid * wide(gain_mid)).astype(bf16)
    hidden_part = dot_nn(scaled_mid, ff_in[...])
    piece = hidden_part.shape[1] // n_kv
    for k in range(n_kv):
        part_ff[k] = hidden_part[:, k * piece : (k + 1) * piece]
    finish = begin("kv", lambda k: part_ff.at[k], lambda k: got_ff.at[k])
    got_ff[kv] = part_ff[kv]
    finish_stat()
    inv_mid = lax.rsqrt(jnp.sum(got_stat[...], axis=0)[:, :1] / d_model + EPS)
    loads[17].wait()
    finish()
    full_ff[kv] = jnp.sum(got_ff[...], axis=0)
    finish = begin("kv", lambda k: full_ff.at[kv], lambda k: full_ff.at[k])
    finish()
    hidden_sum = jnp.concatenate([full_ff[k] for k in range(n_kv)], axis=1)
    hidden = jnp.square(jnp.maximum(inv_mid * hidden_sum, 0.0)).astype(bf16)
    got_mix[tp] = dot_nn(hidden, ff_out[...])
    finish = begin("tp", lambda t: got_mix.at[tp], lambda t: got_mix.at[t])
    finish()
    mixed_ref[...] = (resid_mid + jnp.sum(got_mix[...], axis=0)).astype(bf16)
    for copy in sent:
        copy.wait_send()


def hand_out(mixed, new_latent, new_rope, mixed_out, new_latent_out, new_rope_out):
    mixed_out[...] = mixed[...]
    new_latent_out[...] = new_latent[...]
    new_rope_out[...] = new_rope[...]


def per_device_kernel(
    n_kv, n_tp,
    tokens, lengths, latent_cache, rope_cache, gain_in, w_down_q, w_down_kv, w_rope_key, gain_q,
    w_up_qn, w_up_qr, gain_kv, w_key_up, w_value_up, w_attn_out, gain_mid, w_ff_in, w_ff_out,
):
    f32 = jnp.float32
    bf16 = jnp.bfloat16
    seqs, width = tokens.shape
    q_rank, heads, nope = w_up_qn.shape
    kv_rank, _, v_size = w_value_up.shape
    rope_size = w_rope_key.shape[1]
    hidden = w_ff_in.shape[1]
    own_seqs = seqs // n_kv
    v_wide = heads // n_tp * v_size
    big = [
        tokens,
        gain_in,
        lengths,
        gain_q,
        gain_kv,
        gain_mid,
        latent_cache,
        rope_cache.transpose(0, 2, 1),
        w_down_q,
        w_down_kv,
        w_rope_key.T,
        w_up_qn.transpose(1, 2, 0).reshape(heads * nope, q_rank),
        w_up_qr.transpose(1, 2, 0).reshape(heads * rope_size, q_rank),
        w_key_up.transpose(1, 2, 0),
        w_value_up.transpose(1, 2, 0),
        w_attn_out.reshape(-1, width),
        w_ff_in,
        w_ff_out,
    ]
    block = (q_rank + kv_rank + 2 * LANES) // n_tp
    messages = 6 * (n_kv - 1) + 4 * (n_tp - 1)
    vmem = pltpu.VMEM
    whole = pl.BlockSpec(memory_space=pltpu.VMEM)
    results = pl.pallas_call(
        functools.partial(layer_kernel, n_kv, n_tp),
        out_shape=(
            jax.ShapeDtypeStruct((seqs, width), bf16),
            jax.ShapeDtypeStruct((seqs, kv_rank), bf16),
            jax.ShapeDtypeStruct((seqs, rope_size), bf16),
        ),
        in_specs=[pl.BlockSpec(memory_space=pl.ANY)] * len(big),
        out_specs=(whole, whole, whole),
        scratch_shapes=[
            pltpu.SMEM(a.shape, a.dtype) if a is lengths else vmem(a.shape, a.dtype) for a in big
        ]
        + [
            vmem((n_tp, seqs, block), f32),
            vmem((n_kv, seqs, block), f32),
            vmem((n_tp, seqs, block), f32),
            vmem((heads, seqs, kv_rank), f32),
            vmem((heads, seqs, rope_size), f32),
            vmem((seqs, heads, kv_rank + 2 * LANES), f32),
            vmem((n_tp, seqs, v_wide + LANES), f32),
            vmem((n_tp, seqs, v_wide + LANES), f32),
            vmem((n_kv, own_seqs, v_wide + LANES), f32),
            vmem((n_kv, own_seqs, v_wide + LANES), f32),
            vmem((n_kv, own_seqs, v_wide), f32),
            vmem((n_tp, seqs, width), f32),
            vmem((n_kv, seqs, LANES), f32),
            vmem((n_kv, seqs, hidden // n_kv), f32),
            vmem((n_kv, seqs, hidden // n_kv), f32),
            vmem((n_kv, seqs, hidden // n_kv), f32),
            vmem((n_tp, seqs, width), f32),
            pltpu.SemaphoreType.DMA((len(big),)),
            pltpu.SemaphoreType.DMA((messages,)),
            pltpu.SemaphoreType.DMA((messages,)),
        ],
        compiler_params=pltpu.CompilerParams(collective_id=0, has_side_effects=True),
        name="layer",
    )(*big)
    return pl.pallas_call(
        hand_out,
        out_shape=tuple(jax.ShapeDtypeStruct(a.shape, a.dtype) for a in results),
        in_specs=[whole] * 3,
        out_specs=(whole,) * 3,
        name="hand_out",
    )(*results)


def kernel_fits(n_kv, n_tp, seqs, width, q_rank, kv_rank, rope_size, heads, v_size, hidden):
    return (
        seqs % n_kv == 0
        and heads % n_tp == 0
        and width % LANES == 0
        and q_rank % LANES == 0
        and kv_rank % LANES == 0
        and LANES % rope_size == 0
        and (heads * rope_size) % LANES == 0
        and (q_rank + kv_rank + 2 * LANES) % (n_tp * LANES) == 0
        and (heads // n_tp * v_size) % LANES == 0
        and hidden % (n_kv * LANES) == 0
    )


def per_device_any(n_kv, n_tp, *args):
    tokens, w_down_q, w_down_kv, w_rope_key = args[0], args[5], args[6], args[7]
    w_value_up, w_ff_in = args[13], args[16]
    if kernel_fits(
        n_kv, n_tp, *tokens.shape, w_down_q.shape[1], w_down_kv.shape[1], w_rope_key.shape[1],
        *w_value_up.shape[1:], w_ff_in.shape[1],
    ):
        return per_device_kernel(n_kv, n_tp, *args)
    return per_device(*args)


def solution(mesh):
    return jax.shard_map(
        functools.partial(per_device_any, mesh.shape["kv"], mesh.shape["tp"]),
        mesh=mesh,
        in_specs=(
            P(None, "kv"),
            P(),
            P(None, ("kv", "tp"), None),
            P(None, ("kv", "tp"), None),
            P("kv"),
            P("kv", None),
            P("kv", None),
            P("kv", None),
            P(),
            P(),
            P(),
            P(),
            P(),
            P(),
            P("tp", None, "kv"),
            P("kv"),
            P("kv", "tp"),
            P("tp", "kv"),
        ),
        out_specs=(P(None, "kv"), P(), P()),
        check_vma=False,
    )
```

```python
import functools

import jax
import jax.numpy as jnp
from jax import lax
from jax.experimental import pallas as pl
from jax.experimental.pallas import tpu as pltpu
from jax.sharding import PartitionSpec as P

D = 2048
NOPE = 64
ROPE = 32


EPS = 1e-06


def combined_all(part, axis, combine):
    gathered = jax.tree.map(lambda a: lax.all_gather(a, axis), part)

    def take(source):
        return jax.tree.map(lambda a: lax.dynamic_index_in_dim(a, source, 0, False), gathered)

    return lax.fori_loop(
        1, lax.axis_size(axis), lambda source, state: combine(state, take(source)), take(0)
    )


def rotate(values, positions):
    half = values.shape[-1] // 2
    inverse = 10000.0 ** (-jnp.arange(half, dtype=jnp.float32) / half)
    angle = positions.astype(jnp.float32)[:, None, None] * inverse[None, None, :]
    first = values[..., :half]
    second = values[..., half:]
    return jnp.concatenate(
        [
            first * jnp.cos(angle) - second * jnp.sin(angle),
            second * jnp.cos(angle) + first * jnp.sin(angle),
        ],
        axis=-1,
    )


def rms_scaled(values, gain):
    return (
        values
        * lax.rsqrt(jnp.mean(values * values, axis=-1, keepdims=True) + EPS)
        * gain.astype(jnp.float32)
    )


def combine(earlier, later):
    top_a, total_a, acc_a = earlier
    top_b, total_b, acc_b = later
    top = jnp.maximum(top_a, top_b)
    fade_a = jnp.exp(top_a - top)
    fade_b = jnp.exp(top_b - top)
    return (
        top,
        total_a * fade_a + total_b * fade_b,
        acc_a * fade_a[..., None] + acc_b * fade_b[..., None],
    )


def fold_sources(parts):
    tops, totals, accs = parts
    top = jnp.max(tops, axis=0)
    fade = jnp.exp(tops - top[None])
    return (top, jnp.sum(totals * fade, axis=0), jnp.sum(accs * fade[..., None], axis=0))


def per_device(
    tokens,
    lengths,
    latent_cache,
    rope_cache,
    gain_in,
    w_down_q,
    w_down_kv,
    w_rope_key,
    gain_q,
    w_up_qn,
    w_up_qr,
    gain_kv,
    w_key_up,
    w_value_up,
    w_attn_out,
    gain_mid,
    w_ff_in,
    w_ff_out,
):
    f32 = jnp.float32
    bf16 = jnp.bfloat16
    highest = lax.Precision.HIGHEST
    scale = (NOPE + ROPE) ** (-0.5)
    resid = tokens.astype(f32)
    scaled_in = (resid * gain_in.astype(f32)).astype(bf16)
    part_q = jnp.dot(scaled_in, w_down_q, preferred_element_type=f32)
    part_kv = jnp.dot(scaled_in, w_down_kv, preferred_element_type=f32)
    part_rope = jnp.dot(scaled_in, w_rope_key, preferred_element_type=f32)
    square_in = jnp.sum(resid * resid, axis=1)
    sum_q, sum_kv, sum_rope, total_in = lax.psum((part_q, part_kv, part_rope, square_in), "kv")
    inv_in = lax.rsqrt(total_in / D + EPS)[:, None]
    query_latent = rms_scaled(inv_in * sum_q, gain_q).astype(bf16)
    new_latent = rms_scaled(inv_in * sum_kv, gain_kv).astype(bf16)
    new_rope_key = rotate((inv_in * sum_rope)[:, None, :], lengths)[:, 0, :].astype(bf16)
    query_nope = jnp.einsum(
        "bc,chd->bhd", query_latent, w_up_qn, preferred_element_type=f32
    ).astype(bf16)
    query_rope = rotate(
        jnp.einsum("bc,chr->bhr", query_latent, w_up_qr, preferred_element_type=f32), lengths
    ).astype(bf16)
    query_cache = jnp.einsum(
        "bhd,khd->bhk", query_nope, w_key_up, preferred_element_type=f32
    ).astype(bf16)
    rows = latent_cache.shape[1]
    positions = lax.axis_index(("kv", "tp")) * rows + jnp.arange(rows, dtype=jnp.int32)
    live = (positions[None, :] < lengths[:, None])[:, None, :]
    scores = (
        jnp.einsum("bhk,blk->bhl", query_cache, latent_cache, preferred_element_type=f32)
        + jnp.einsum("bhr,blr->bhl", query_rope, rope_cache, preferred_element_type=f32)
    ) * scale
    scores = jnp.where(live, scores, -1e30)
    top = jnp.max(scores, axis=2)
    weights = jnp.where(live, jnp.exp(scores - top[:, :, None]), 0.0)
    total = jnp.sum(weights, axis=2)
    acc = jnp.einsum("bhl,blk->bhk", weights.astype(bf16), latent_cache, preferred_element_type=f32)
    heads_dev = w_attn_out.shape[0]
    first_head = lax.axis_index("tp") * heads_dev
    own_value_up = lax.dynamic_slice_in_dim(w_value_up, first_head, heads_dev, 1).astype(f32)
    own_cache_q = lax.dynamic_slice_in_dim(query_cache, first_head, heads_dev, 1)
    own_rope_q = lax.dynamic_slice_in_dim(query_rope, first_head, heads_dev, 1)
    self_score = (
        jnp.einsum("bhk,bk->bh", own_cache_q, new_latent, preferred_element_type=f32)
        + jnp.einsum("bhr,br->bh", own_rope_q, new_rope_key, preferred_element_type=f32)
    ) * scale
    top, total, acc = fold_sources(
        (
            lax.all_to_all(top[None], "tp", split_axis=2, concat_axis=0, tiled=True),
            lax.all_to_all(total[None], "tp", split_axis=2, concat_axis=0, tiled=True),
            lax.all_to_all(acc[None], "tp", split_axis=2, concat_axis=0, tiled=True),
        )
    )
    top, total, acc = combined_all((top, total, acc), "kv", combine)
    joined = jnp.maximum(top, self_score)
    fade = jnp.exp(top - joined)
    self_weight = jnp.exp(self_score - joined)
    total = total * fade + self_weight
    acc = (
        acc * fade[:, :, None]
        + self_weight.astype(bf16).astype(f32)[:, :, None] * new_latent.astype(f32)[:, None, :]
    )
    expanded = jnp.einsum("bhk,khv->bhv", acc, own_value_up, precision=highest)
    head_out = (expanded / total[:, :, None]).astype(bf16)
    attn_part = jnp.einsum("bhv,hvd->bd", head_out, w_attn_out, preferred_element_type=f32)
    resid_mid = resid + lax.psum(attn_part, "tp")
    scaled_mid = (resid_mid * gain_mid.astype(f32)).astype(bf16)
    hidden_part = jnp.dot(scaled_mid, w_ff_in, preferred_element_type=f32)
    square_mid = jnp.sum(resid_mid * resid_mid, axis=1)
    hidden_sum, total_mid = lax.psum((hidden_part, square_mid), "kv")
    inv_mid = lax.rsqrt(total_mid / D + EPS)[:, None]
    hidden = jnp.square(jax.nn.relu(inv_mid * hidden_sum)).astype(bf16)
    out_part = jnp.dot(hidden, w_ff_out, preferred_element_type=f32)
    mixed = (resid_mid + lax.psum(out_part, "tp")).astype(bf16)
    return (mixed, new_latent, new_rope_key)

MESH = pl.DeviceIdType.MESH
LANES = 128


def dot_nt(a, b):
    return lax.dot_general(a, b, (((1,), (1,)), ((), ())), preferred_element_type=jnp.float32)


def dot_nn(a, b):
    return jnp.dot(a, b, preferred_element_type=jnp.float32)


def turn(values, cos, sin, half):
    width = values.shape[1]
    lane = lax.broadcasted_iota(jnp.int32, values.shape, 1)
    partner = jnp.where(
        lane % (2 * half) < half,
        -pltpu.roll(values, width - half, 1),
        pltpu.roll(values, half, 1),
    )
    return values * cos + partner * sin


def layer_kernel(
    n_kv, n_tp,
    tokens_h, gain_in_h, lengths_h, gain_q_h, gain_kv_h, gain_mid_h,
    latent_h, rope_h, down_q_h, down_kv_h, down_r_h, up_qn_h, up_qr_h, key_up_h, value_up_h,
    attn_out_h, ff_in_h, ff_out_h,
    mixed_ref, new_latent_ref, new_rope_ref,
    tokens, gain_in, lengths, gain_q, gain_kv, gain_mid,
    latent, rope, down_q, down_kv, down_r, up_qn, up_qr, key_up, value_up, attn_out, ff_in, ff_out,
    part_in, got_in, full_in, q_rows, r_rows, acc_rows, part_att, got_att, got_top, got_seq,
    got_out, got_stat, part_ff, got_ff, full_ff, got_mix,
    load_sem, send_sem, recv_sem,
):
    f32 = jnp.float32
    bf16 = jnp.bfloat16
    kv = lax.axis_index("kv")
    tp = lax.axis_index("tp")
    me = kv * n_tp + tp
    loads = [
        pltpu.make_async_copy(src, dst, load_sem.at[i])
        for i, (src, dst) in enumerate((
            (tokens_h, tokens), (gain_in_h, gain_in), (down_q_h, down_q), (down_kv_h, down_kv),
            (down_r_h, down_r), (lengths_h, lengths), (gain_q_h, gain_q), (gain_kv_h, gain_kv),
            (gain_mid_h, gain_mid), (up_qn_h, up_qn), (up_qr_h, up_qr), (key_up_h, key_up),
            (latent_h, latent), (rope_h, rope), (value_up_h, value_up), (attn_out_h, attn_out),
            (ff_in_h, ff_in), (ff_out_h, ff_out),
        ))
    ]
    for copy in loads[:9]:
        copy.start()

    barrier = pltpu.get_barrier_semaphore()
    peers = [(lax.rem(kv + d, n_kv), tp) for d in range(1, n_kv)]
    peers += [(kv, lax.rem(tp + d, n_tp)) for d in range(1, n_tp)]
    for peer in peers:
        pl.semaphore_signal(barrier, inc=1, device_id=peer, device_id_type=MESH)

    def remote(src, dst, slot, where):
        return pltpu.make_async_remote_copy(
            src_ref=src, dst_ref=dst, send_sem=send_sem.at[slot], recv_sem=recv_sem.at[slot],
            device_id=where, device_id_type=MESH,
        )

    sent = []
    slots = [0]

    def begin(axis, src_of, dst_of, group=None, prepare=None):
        count, mine = {"kv": (n_kv, kv), "tp": (n_tp, tp)}[axis]
        base = slots[0]
        slots[0] += count - 1

        def where(index):
            return (index, tp) if axis == "kv" else (kv, index)

        arriving = []
        steps = sorted(range(1, count), key=lambda d: -min(d, count - d))
        for i, d in enumerate(steps):
            if prepare is not None and i % group == 0:
                for ahead in steps[i : i + group]:
                    prepare(lax.rem(mine + ahead, count))
            peer = lax.rem(mine + d, count)
            copy = remote(src_of(peer), dst_of(mine), base + d - 1, where(peer))
            copy.start()
            sent.append(copy)
            source = lax.rem(mine + count - d, count)
            landed = remote(dst_of(source), dst_of(source), base + d - 1, where(source))
            arriving.append((source, landed))

        def finish(use=None):
            for source, copy in reversed(arriving):
                copy.wait_recv()
                if use is not None:
                    use(source)

        return finish

    seqs, width = tokens.shape
    q_rank = down_q.shape[1]
    kv_rank = down_kv.shape[1]
    rope_size = down_r.shape[0]
    half = rope_size // 2
    heads = key_up.shape[0]
    nope = key_up.shape[1]
    v_size = value_up.shape[1]
    rows = latent.shape[1]
    own_heads = heads // n_tp
    scale = (nope + rope_size) ** (-0.5)
    d_model = width * n_kv

    def wide(gain):
        return gain[...].astype(f32)[None, :]

    def across(values):
        spare = jnp.zeros((LANES - values.shape[0], LANES), f32)
        return jnp.transpose(jnp.concatenate([values, spare], axis=0))

    for copy in loads[:5]:
        copy.wait()
    for copy in loads[9:]:
        copy.start()
    resid = tokens[...].astype(f32)
    scaled_in = (resid * wide(gain_in)).astype(bf16)
    square = jnp.sum(resid * resid, axis=1, keepdims=True)
    part = jnp.concatenate(
        [
            dot_nn(scaled_in, down_q[...]),
            dot_nn(scaled_in, down_kv[...]),
            dot_nt(scaled_in, down_r[...]),
            jnp.zeros((seqs, LANES - rope_size), f32),
            jnp.broadcast_to(square, (seqs, LANES)),
        ],
        axis=1,
    )
    block = part.shape[1] // n_tp
    for i in range(n_tp):
        part_in[i] = part[:, i * block : (i + 1) * block]
    pl.semaphore_wait(barrier, len(peers))
    finish = begin("kv", lambda k: part_in.at[tp], lambda k: got_in.at[k])
    got_in[kv] = part_in[tp]

    for copy in loads[5:9]:
        copy.wait()
    lane = lax.broadcasted_iota(jnp.int32, (seqs, LANES), 1)
    row = lax.broadcasted_iota(jnp.int32, (seqs, LANES), 0)
    where_at = jnp.zeros((seqs, LANES), jnp.int32)
    for b in range(seqs):
        where_at = jnp.where(row == b, lengths[b], where_at)
    inverse = jnp.zeros((seqs, LANES), f32)
    for j in range(half):
        inverse = jnp.where(lane % half == j, 10000.0 ** (-j / half), inverse)
    angle = where_at.astype(f32) * inverse
    cos, sin = jnp.cos(angle), jnp.sin(angle)
    finish()
    full_in[tp] = jnp.sum(got_in[...], axis=0)
    finish = begin("tp", lambda t: full_in.at[tp], lambda t: full_in.at[t])
    for copy in loads[9:12]:
        copy.wait()
    finish()
    sums = jnp.concatenate([full_in[i] for i in range(n_tp)], axis=1)
    inv_in = lax.rsqrt(sums[:, q_rank + kv_rank + LANES :][:, :1] / d_model + EPS)
    lat_q = inv_in * sums[:, :q_rank]
    query_latent = (
        lat_q
        * lax.rsqrt(jnp.mean(lat_q * lat_q, axis=1, keepdims=True) + EPS)
        * wide(gain_q)
    ).astype(bf16)
    lat_kv = inv_in * sums[:, q_rank : q_rank + kv_rank]
    new_latent = (
        lat_kv
        * lax.rsqrt(jnp.mean(lat_kv * lat_kv, axis=1, keepdims=True) + EPS)
        * wide(gain_kv)
    ).astype(bf16)
    new_latent_ref[...] = new_latent
    new_latent = new_latent.astype(f32)
    new_rope = turn(
        inv_in * sums[:, q_rank + kv_rank : q_rank + kv_rank + LANES], cos, sin, half
    ).astype(bf16)
    new_rope_ref[...] = new_rope[:, :rope_size]
    new_rope = new_rope.astype(f32)[:, :rope_size]

    query_nope = dot_nt(query_latent, up_qn[...]).astype(bf16)
    times = heads * rope_size // LANES
    query_rope = turn(
        dot_nt(query_latent, up_qr[...]),
        jnp.concatenate([cos] * times, axis=1),
        jnp.concatenate([sin] * times, axis=1),
        half,
    ).astype(bf16).astype(f32)
    for h in range(heads):
        q_rows[h] = dot_nn(query_nope[:, h * nope : (h + 1) * nope], key_up[h]).astype(
            bf16
        ).astype(f32)
        r_rows[h] = query_rope[:, h * rope_size : (h + 1) * rope_size]

    for copy in loads[12:15]:
        copy.wait()
    first = me * rows
    at = first + lax.broadcasted_iota(jnp.int32, (heads, rows), 1)
    scores, selfs, lives = [], [], []
    for b in range(seqs):
        q_b = q_rows[:, b, :]
        r_b = r_rows[:, b, :]
        score = (
            dot_nt(q_b.astype(bf16), latent[b]) + dot_nn(r_b.astype(bf16), rope[b])
        ) * scale
        live = at < lengths[b]
        scores.append(jnp.where(live, score, -1e30))
        lives.append(live)
        own = (
            jnp.sum(q_b * new_latent[b : b + 1, :], axis=1, keepdims=True)
            + jnp.sum(r_b * new_rope[b : b + 1, :], axis=1, keepdims=True)
        ) * scale
        selfs.append(own)
    mine = me == 0
    for b in range(seqs):
        own = jnp.where(mine, selfs[b], -1e30)
        top = jnp.maximum(jnp.max(scores[b], axis=1, keepdims=True), own)
        weights = jnp.where(lives[b], jnp.exp(scores[b] - top), 0.0)
        own_weight = jnp.where(mine, jnp.exp(own - top), 0.0)
        total = jnp.sum(weights, axis=1, keepdims=True) + own_weight
        acc_rows[b, :, :kv_rank] = (
            dot_nn(weights.astype(bf16), latent[b])
            + own_weight.astype(bf16).astype(f32) * new_latent[b : b + 1, :]
        )
        acc_rows[b, :, kv_rank : kv_rank + LANES] = jnp.broadcast_to(top, (heads, LANES))
        acc_rows[b, :, kv_rank + LANES :] = jnp.broadcast_to(total, (heads, LANES))

    v_wide = own_heads * v_size
    for t in range(n_tp):
        pieces = []
        stat = jnp.zeros((seqs, LANES), f32)
        for i in range(own_heads):
            h = t * own_heads + i
            acc = acc_rows[:, h, :]
            exact = acc[:, :kv_rank]
            high = exact.astype(bf16)
            low = (exact - high.astype(f32)).astype(bf16)
            both = dot_nt(jnp.concatenate([high, low], axis=0), value_up[h])
            pieces.append(both[:seqs] + both[seqs:])
            stat = jnp.where(lane == i, acc[:, kv_rank : kv_rank + LANES], stat)
            stat = jnp.where(lane == own_heads + i, acc[:, kv_rank + LANES :], stat)
        part_att[t] = jnp.concatenate(pieces + [stat], axis=1)
    finish = begin("tp", lambda t: part_att.at[t], lambda t: got_att.at[t])
    got_att[tp] = part_att[tp]
    finish()

    stats = [got_att[t][:, v_wide:] for t in range(n_tp)]
    top = functools.reduce(jnp.maximum, stats)
    head_lane = lax.broadcasted_iota(jnp.int32, (seqs, v_wide), 1) // v_size
    joined = jnp.zeros((seqs, v_wide), f32)
    totals = jnp.zeros((seqs, LANES), f32)
    for t in range(n_tp):
        fade_t = jnp.exp(stats[t] - top)
        fade = jnp.zeros((seqs, v_wide), f32)
        for i in range(own_heads):
            fade = jnp.where(head_lane == i, fade_t[:, i : i + 1], fade)
        joined += got_att[t][:, :v_wide] * fade
        totals += stats[t] * pltpu.roll(fade_t, own_heads, 1)
    got_top[kv] = across(jnp.where(lane < own_heads, top, totals))[: got_top.shape[1], :]
    got_seq[kv] = joined
    finish_top = begin("kv", lambda k: got_top.at[kv], lambda k: got_top.at[k])
    finish = begin("kv", lambda k: got_seq.at[kv], lambda k: got_seq.at[k])
    loads[15].wait()
    finish_top()
    tops = [got_top[k][:own_heads, :] for k in range(n_kv)]
    top = functools.reduce(jnp.maximum, tops)
    fades = [jnp.exp(tops[k] - top) for k in range(n_kv)]
    total = sum(got_top[k][own_heads : 2 * own_heads, :] * fades[k] for k in range(n_kv))
    used = lax.broadcasted_iota(jnp.int32, total.shape, 1) < seqs
    share = 1.0 / jnp.where(used, total, 1.0)
    shares = across(jnp.concatenate([fade * share for fade in fades], axis=0))[:seqs, :]
    finish()
    head_sum = jnp.zeros((seqs, v_wide), f32)
    for k in range(n_kv):
        fade = jnp.zeros((seqs, v_wide), f32)
        for i in range(own_heads):
            at_lane = k * own_heads + i
            fade = jnp.where(head_lane == i, shares[:, at_lane : at_lane + 1], fade)
        head_sum += got_seq[k] * fade
    head_out = head_sum.astype(bf16)

    got_out[tp] = dot_nn(head_out, attn_out[...])
    finish = begin("tp", lambda t: got_out.at[tp], lambda t: got_out.at[t])
    loads[16].wait()
    finish()
    resid_mid = resid + jnp.sum(got_out[...], axis=0)
    got_stat[kv] = jnp.broadcast_to(
        jnp.sum(resid_mid * resid_mid, axis=1, keepdims=True), (seqs, LANES)
    )
    finish_stat = begin("kv", lambda k: got_stat.at[kv], lambda k: got_stat.at[k])
    scaled_mid = (resid_mid * wide(gain_mid)).astype(bf16)
    piece = ff_in.shape[1] // n_kv

    def hidden_of(k):
        columns = pl.ds(pl.multiple_of(k * piece, LANES), piece)
        return dot_nn(scaled_mid, ff_in[:, columns])

    def prepare(k):
        part_ff[k] = hidden_of(k)

    finish = begin("kv", lambda k: part_ff.at[k], lambda k: got_ff.at[k], n_kv // 2, prepare)
    got_ff[kv] = hidden_of(kv)
    finish_stat()
    inv_mid = lax.rsqrt(jnp.sum(got_stat[...], axis=0)[:, :1] / d_model + EPS)
    loads[17].wait()
    finish()
    full_ff[kv] = jnp.sum(got_ff[...], axis=0)
    finish = begin("kv", lambda k: full_ff.at[kv], lambda k: full_ff.at[k])
    out_parts = []

    def use(k):
        hidden = jnp.square(jnp.maximum(inv_mid * full_ff[k], 0.0)).astype(bf16)
        columns = pl.ds(pl.multiple_of(k * piece, LANES), piece)
        out_parts.append(dot_nn(hidden, ff_out[columns, :]))

    use(kv)
    finish(use)
    got_mix[tp] = sum(out_parts)
    finish = begin("tp", lambda t: got_mix.at[tp], lambda t: got_mix.at[t])
    finish()
    mixed_ref[...] = (resid_mid + jnp.sum(got_mix[...], axis=0)).astype(bf16)
    for copy in sent:
        copy.wait_send()


def hand_out(mixed, new_latent, new_rope, mixed_out, new_latent_out, new_rope_out):
    mixed_out[...] = mixed[...]
    new_latent_out[...] = new_latent[...]
    new_rope_out[...] = new_rope[...]


def per_device_kernel(
    n_kv, n_tp,
    tokens, lengths, latent_cache, rope_cache, gain_in, w_down_q, w_down_kv, w_rope_key, gain_q,
    w_up_qn, w_up_qr, gain_kv, w_key_up, w_value_up, w_attn_out, gain_mid, w_ff_in, w_ff_out,
):
    f32 = jnp.float32
    bf16 = jnp.bfloat16
    seqs, width = tokens.shape
    q_rank, heads, nope = w_up_qn.shape
    kv_rank, _, v_size = w_value_up.shape
    rope_size = w_rope_key.shape[1]
    hidden = w_ff_in.shape[1]
    v_wide = heads // n_tp * v_size
    top_rows = pl.cdiv(2 * (heads // n_tp), 8) * 8
    big = [
        tokens,
        gain_in,
        lengths,
        gain_q,
        gain_kv,
        gain_mid,
        latent_cache,
        rope_cache.transpose(0, 2, 1),
        w_down_q,
        w_down_kv,
        w_rope_key.T,
        w_up_qn.transpose(1, 2, 0).reshape(heads * nope, q_rank),
        w_up_qr.transpose(1, 2, 0).reshape(heads * rope_size, q_rank),
        w_key_up.transpose(1, 2, 0),
        w_value_up.transpose(1, 2, 0),
        w_attn_out.reshape(-1, width),
        w_ff_in,
        w_ff_out,
    ]
    block = (q_rank + kv_rank + 2 * LANES) // n_tp
    messages = 6 * (n_kv - 1) + 4 * (n_tp - 1)
    vmem = pltpu.VMEM
    whole = pl.BlockSpec(memory_space=pltpu.VMEM)
    results = pl.pallas_call(
        functools.partial(layer_kernel, n_kv, n_tp),
        out_shape=(
            jax.ShapeDtypeStruct((seqs, width), bf16),
            jax.ShapeDtypeStruct((seqs, kv_rank), bf16),
            jax.ShapeDtypeStruct((seqs, rope_size), bf16),
        ),
        in_specs=[pl.BlockSpec(memory_space=pl.ANY)] * len(big),
        out_specs=(whole, whole, whole),
        scratch_shapes=[
            pltpu.SMEM(a.shape, a.dtype) if a is lengths else vmem(a.shape, a.dtype) for a in big
        ]
        + [
            vmem((n_tp, seqs, block), f32),
            vmem((n_kv, seqs, block), f32),
            vmem((n_tp, seqs, block), f32),
            vmem((heads, seqs, kv_rank), f32),
            vmem((heads, seqs, rope_size), f32),
            vmem((seqs, heads, kv_rank + 2 * LANES), f32),
            vmem((n_tp, seqs, v_wide + LANES), f32),
            vmem((n_tp, seqs, v_wide + LANES), f32),
            vmem((n_kv, top_rows, LANES), f32),
            vmem((n_kv, seqs, v_wide), f32),
            vmem((n_tp, seqs, width), f32),
            vmem((n_kv, seqs, LANES), f32),
            vmem((n_kv, seqs, hidden // n_kv), f32),
            vmem((n_kv, seqs, hidden // n_kv), f32),
            vmem((n_kv, seqs, hidden // n_kv), f32),
            vmem((n_tp, seqs, width), f32),
            pltpu.SemaphoreType.DMA((len(big),)),
            pltpu.SemaphoreType.DMA((messages,)),
            pltpu.SemaphoreType.DMA((messages,)),
        ],
        compiler_params=pltpu.CompilerParams(collective_id=0, has_side_effects=True),
        name="layer",
    )(*big)
    return pl.pallas_call(
        hand_out,
        out_shape=tuple(jax.ShapeDtypeStruct(a.shape, a.dtype) for a in results),
        in_specs=[whole] * 3,
        out_specs=(whole,) * 3,
        name="hand_out",
    )(*results)


def kernel_fits(n_kv, n_tp, seqs, width, q_rank, kv_rank, rope_size, heads, v_size, hidden):
    return (
        heads % n_tp == 0
        and seqs <= LANES
        and n_kv * (heads // n_tp) <= LANES
        and width % LANES == 0
        and q_rank % LANES == 0
        and kv_rank % LANES == 0
        and LANES % rope_size == 0
        and (heads * rope_size) % LANES == 0
        and (q_rank + kv_rank + 2 * LANES) % (n_tp * LANES) == 0
        and (heads // n_tp * v_size) % LANES == 0
        and hidden % (n_kv * LANES) == 0
    )


def per_device_any(n_kv, n_tp, *args):
    tokens, w_down_q, w_down_kv, w_rope_key = args[0], args[5], args[6], args[7]
    w_value_up, w_ff_in = args[13], args[16]
    if kernel_fits(
        n_kv, n_tp, *tokens.shape, w_down_q.shape[1], w_down_kv.shape[1], w_rope_key.shape[1],
        *w_value_up.shape[1:], w_ff_in.shape[1],
    ):
        return per_device_kernel(n_kv, n_tp, *args)
    return per_device(*args)


def solution(mesh):
    return jax.shard_map(
        functools.partial(per_device_any, mesh.shape["kv"], mesh.shape["tp"]),
        mesh=mesh,
        in_specs=(
            P(None, "kv"),
            P(),
            P(None, ("kv", "tp"), None),
            P(None, ("kv", "tp"), None),
            P("kv"),
            P("kv", None),
            P("kv", None),
            P("kv", None),
            P(),
            P(),
            P(),
            P(),
            P(),
            P(),
            P("tp", None, "kv"),
            P("kv"),
            P("kv", "tp"),
            P("tp", "kv"),
        ),
        out_specs=(P(None, "kv"), P(), P()),
        check_vma=False,
    )
```

```python
import functools

import jax
import jax.numpy as jnp
from jax import lax
from jax.experimental import pallas as pl
from jax.experimental.pallas import tpu as pltpu
from jax.sharding import PartitionSpec as P

D = 2048
NOPE = 64
ROPE = 32


EPS = 1e-06


def combined_all(part, axis, combine):
    gathered = jax.tree.map(lambda a: lax.all_gather(a, axis), part)

    def take(source):
        return jax.tree.map(lambda a: lax.dynamic_index_in_dim(a, source, 0, False), gathered)

    return lax.fori_loop(
        1, lax.axis_size(axis), lambda source, state: combine(state, take(source)), take(0)
    )


def rotate(values, positions):
    half = values.shape[-1] // 2
    inverse = 10000.0 ** (-jnp.arange(half, dtype=jnp.float32) / half)
    angle = positions.astype(jnp.float32)[:, None, None] * inverse[None, None, :]
    first = values[..., :half]
    second = values[..., half:]
    return jnp.concatenate(
        [
            first * jnp.cos(angle) - second * jnp.sin(angle),
            second * jnp.cos(angle) + first * jnp.sin(angle),
        ],
        axis=-1,
    )


def rms_scaled(values, gain):
    return (
        values
        * lax.rsqrt(jnp.mean(values * values, axis=-1, keepdims=True) + EPS)
        * gain.astype(jnp.float32)
    )


def combine(earlier, later):
    top_a, total_a, acc_a = earlier
    top_b, total_b, acc_b = later
    top = jnp.maximum(top_a, top_b)
    fade_a = jnp.exp(top_a - top)
    fade_b = jnp.exp(top_b - top)
    return (
        top,
        total_a * fade_a + total_b * fade_b,
        acc_a * fade_a[..., None] + acc_b * fade_b[..., None],
    )


def fold_sources(parts):
    tops, totals, accs = parts
    top = jnp.max(tops, axis=0)
    fade = jnp.exp(tops - top[None])
    return (top, jnp.sum(totals * fade, axis=0), jnp.sum(accs * fade[..., None], axis=0))


def per_device(
    tokens,
    lengths,
    latent_cache,
    rope_cache,
    gain_in,
    w_down_q,
    w_down_kv,
    w_rope_key,
    gain_q,
    w_up_qn,
    w_up_qr,
    gain_kv,
    w_key_up,
    w_value_up,
    w_attn_out,
    gain_mid,
    w_ff_in,
    w_ff_out,
):
    f32 = jnp.float32
    bf16 = jnp.bfloat16
    highest = lax.Precision.HIGHEST
    scale = (NOPE + ROPE) ** (-0.5)
    resid = tokens.astype(f32)
    scaled_in = (resid * gain_in.astype(f32)).astype(bf16)
    part_q = jnp.dot(scaled_in, w_down_q, preferred_element_type=f32)
    part_kv = jnp.dot(scaled_in, w_down_kv, preferred_element_type=f32)
    part_rope = jnp.dot(scaled_in, w_rope_key, preferred_element_type=f32)
    square_in = jnp.sum(resid * resid, axis=1)
    sum_q, sum_kv, sum_rope, total_in = lax.psum((part_q, part_kv, part_rope, square_in), "kv")
    inv_in = lax.rsqrt(total_in / D + EPS)[:, None]
    query_latent = rms_scaled(inv_in * sum_q, gain_q).astype(bf16)
    new_latent = rms_scaled(inv_in * sum_kv, gain_kv).astype(bf16)
    new_rope_key = rotate((inv_in * sum_rope)[:, None, :], lengths)[:, 0, :].astype(bf16)
    query_nope = jnp.einsum(
        "bc,chd->bhd", query_latent, w_up_qn, preferred_element_type=f32
    ).astype(bf16)
    query_rope = rotate(
        jnp.einsum("bc,chr->bhr", query_latent, w_up_qr, preferred_element_type=f32), lengths
    ).astype(bf16)
    query_cache = jnp.einsum(
        "bhd,khd->bhk", query_nope, w_key_up, preferred_element_type=f32
    ).astype(bf16)
    rows = latent_cache.shape[1]
    positions = lax.axis_index(("kv", "tp")) * rows + jnp.arange(rows, dtype=jnp.int32)
    live = (positions[None, :] < lengths[:, None])[:, None, :]
    scores = (
        jnp.einsum("bhk,blk->bhl", query_cache, latent_cache, preferred_element_type=f32)
        + jnp.einsum("bhr,blr->bhl", query_rope, rope_cache, preferred_element_type=f32)
    ) * scale
    scores = jnp.where(live, scores, -1e30)
    top = jnp.max(scores, axis=2)
    weights = jnp.where(live, jnp.exp(scores - top[:, :, None]), 0.0)
    total = jnp.sum(weights, axis=2)
    acc = jnp.einsum("bhl,blk->bhk", weights.astype(bf16), latent_cache, preferred_element_type=f32)
    heads_dev = w_attn_out.shape[0]
    first_head = lax.axis_index("tp") * heads_dev
    own_value_up = lax.dynamic_slice_in_dim(w_value_up, first_head, heads_dev, 1).astype(f32)
    own_cache_q = lax.dynamic_slice_in_dim(query_cache, first_head, heads_dev, 1)
    own_rope_q = lax.dynamic_slice_in_dim(query_rope, first_head, heads_dev, 1)
    self_score = (
        jnp.einsum("bhk,bk->bh", own_cache_q, new_latent, preferred_element_type=f32)
        + jnp.einsum("bhr,br->bh", own_rope_q, new_rope_key, preferred_element_type=f32)
    ) * scale
    top, total, acc = fold_sources(
        (
            lax.all_to_all(top[None], "tp", split_axis=2, concat_axis=0, tiled=True),
            lax.all_to_all(total[None], "tp", split_axis=2, concat_axis=0, tiled=True),
            lax.all_to_all(acc[None], "tp", split_axis=2, concat_axis=0, tiled=True),
        )
    )
    top, total, acc = combined_all((top, total, acc), "kv", combine)
    joined = jnp.maximum(top, self_score)
    fade = jnp.exp(top - joined)
    self_weight = jnp.exp(self_score - joined)
    total = total * fade + self_weight
    acc = (
        acc * fade[:, :, None]
        + self_weight.astype(bf16).astype(f32)[:, :, None] * new_latent.astype(f32)[:, None, :]
    )
    expanded = jnp.einsum("bhk,khv->bhv", acc, own_value_up, precision=highest)
    head_out = (expanded / total[:, :, None]).astype(bf16)
    attn_part = jnp.einsum("bhv,hvd->bd", head_out, w_attn_out, preferred_element_type=f32)
    resid_mid = resid + lax.psum(attn_part, "tp")
    scaled_mid = (resid_mid * gain_mid.astype(f32)).astype(bf16)
    hidden_part = jnp.dot(scaled_mid, w_ff_in, preferred_element_type=f32)
    square_mid = jnp.sum(resid_mid * resid_mid, axis=1)
    hidden_sum, total_mid = lax.psum((hidden_part, square_mid), "kv")
    inv_mid = lax.rsqrt(total_mid / D + EPS)[:, None]
    hidden = jnp.square(jax.nn.relu(inv_mid * hidden_sum)).astype(bf16)
    out_part = jnp.dot(hidden, w_ff_out, preferred_element_type=f32)
    mixed = (resid_mid + lax.psum(out_part, "tp")).astype(bf16)
    return (mixed, new_latent, new_rope_key)

MESH = pl.DeviceIdType.MESH
LANES = 128


def dot_nt(a, b):
    return lax.dot_general(a, b, (((1,), (1,)), ((), ())), preferred_element_type=jnp.float32)


def dot_nn(a, b):
    return jnp.dot(a, b, preferred_element_type=jnp.float32)


def turn(values, cos, sin, half):
    width = values.shape[1]
    lane = lax.broadcasted_iota(jnp.int32, values.shape, 1)
    partner = jnp.where(
        lane % (2 * half) < half,
        -pltpu.roll(values, width - half, 1),
        pltpu.roll(values, half, 1),
    )
    return values * cos + partner * sin


def layer_kernel(
    n_kv, n_tp,
    tokens_h, gain_in_h, lengths_h, gain_q_h, gain_kv_h, gain_mid_h,
    latent_h, rope_h, down_q_h, down_kv_h, down_r_h, up_qn_h, up_qr_h, key_up_h, value_up_h,
    attn_out_h, ff_in_h, ff_out_h,
    mixed_ref, new_latent_ref, new_rope_ref,
    tokens, gain_in, lengths, gain_q, gain_kv, gain_mid,
    latent, rope, down_q, down_kv, down_r, up_qn, up_qr, key_up, value_up, attn_out, ff_in, ff_out,
    part_in, got_in, full_in, q_rows, r_rows, acc_rows, part_att, got_att, got_top, got_seq,
    got_out, got_stat, part_ff, got_ff, full_ff, got_mix,
    load_sem, send_sem, recv_sem,
):
    f32 = jnp.float32
    bf16 = jnp.bfloat16
    kv = lax.axis_index("kv")
    tp = lax.axis_index("tp")
    me = kv * n_tp + tp
    loads = [
        pltpu.make_async_copy(src, dst, load_sem.at[i])
        for i, (src, dst) in enumerate((
            (tokens_h, tokens), (gain_in_h, gain_in), (down_q_h, down_q), (down_kv_h, down_kv),
            (down_r_h, down_r), (lengths_h, lengths), (gain_q_h, gain_q), (gain_kv_h, gain_kv),
            (gain_mid_h, gain_mid), (up_qn_h, up_qn), (up_qr_h, up_qr), (key_up_h, key_up),
            (latent_h, latent), (rope_h, rope), (value_up_h, value_up), (attn_out_h, attn_out),
            (ff_in_h, ff_in), (ff_out_h, ff_out),
        ))
    ]
    for copy in loads[:9]:
        copy.start()

    barrier = pltpu.get_barrier_semaphore()
    peers = [(lax.rem(kv + d, n_kv), tp) for d in range(1, n_kv)]
    peers += [(kv, lax.rem(tp + d, n_tp)) for d in range(1, n_tp)]
    for peer in peers:
        pl.semaphore_signal(barrier, inc=1, device_id=peer, device_id_type=MESH)

    def remote(src, dst, slot, where):
        return pltpu.make_async_remote_copy(
            src_ref=src, dst_ref=dst, send_sem=send_sem.at[slot], recv_sem=recv_sem.at[slot],
            device_id=where, device_id_type=MESH,
        )

    sent = []
    slots = [0]

    def begin(axis, src_of, dst_of, group=None, prepare=None):
        count, mine = {"kv": (n_kv, kv), "tp": (n_tp, tp)}[axis]
        base = slots[0]
        slots[0] += count - 1

        def where(index):
            return (index, tp) if axis == "kv" else (kv, index)

        arriving = []
        steps = sorted(range(1, count), key=lambda d: -min(d, count - d))
        for i, d in enumerate(steps):
            if prepare is not None and i % group == 0:
                for ahead in steps[i : i + group]:
                    prepare(lax.rem(mine + ahead, count))
            peer = lax.rem(mine + d, count)
            copy = remote(src_of(peer), dst_of(mine), base + d - 1, where(peer))
            copy.start()
            sent.append(copy)
            source = lax.rem(mine + count - d, count)
            landed = remote(dst_of(source), dst_of(source), base + d - 1, where(source))
            arriving.append((source, landed))

        def finish(use=None):
            for source, copy in reversed(arriving):
                copy.wait_recv()
                if use is not None:
                    use(source)

        return finish

    seqs, width = tokens.shape
    q_rank = down_q.shape[1]
    kv_rank = down_kv.shape[1]
    rope_size = down_r.shape[0]
    half = rope_size // 2
    heads = key_up.shape[0]
    nope = key_up.shape[1]
    v_size = value_up.shape[1]
    rows = latent.shape[1]
    own_heads = heads // n_tp
    scale = (nope + rope_size) ** (-0.5)
    d_model = width * n_kv

    def wide(gain):
        return gain[...].astype(f32)[None, :]

    def across(values):
        spare = jnp.zeros((LANES - values.shape[0], LANES), f32)
        return jnp.transpose(jnp.concatenate([values, spare], axis=0))

    for copy in loads[:5]:
        copy.wait()
    for copy in loads[9:]:
        copy.start()
    resid = tokens[...].astype(f32)
    scaled_in = (resid * wide(gain_in)).astype(bf16)
    square = jnp.sum(resid * resid, axis=1, keepdims=True)
    part = jnp.concatenate(
        [
            dot_nn(scaled_in, down_q[...]),
            dot_nn(scaled_in, down_kv[...]),
            dot_nt(scaled_in, down_r[...]),
            jnp.zeros((seqs, LANES - rope_size), f32),
            jnp.broadcast_to(square, (seqs, LANES)),
        ],
        axis=1,
    )
    block = part.shape[1] // n_tp
    for i in range(n_tp):
        part_in[i] = part[:, i * block : (i + 1) * block]
    pl.semaphore_wait(barrier, len(peers))
    finish = begin("kv", lambda k: part_in.at[tp], lambda k: got_in.at[k])
    got_in[kv] = part_in[tp]

    for copy in loads[5:9]:
        copy.wait()
    lane = lax.broadcasted_iota(jnp.int32, (seqs, LANES), 1)
    row = lax.broadcasted_iota(jnp.int32, (seqs, LANES), 0)
    where_at = jnp.zeros((seqs, LANES), jnp.int32)
    for b in range(seqs):
        where_at = jnp.where(row == b, lengths[b], where_at)
    inverse = jnp.zeros((seqs, LANES), f32)
    for j in range(half):
        inverse = jnp.where(lane % half == j, 10000.0 ** (-j / half), inverse)
    angle = where_at.astype(f32) * inverse
    cos, sin = jnp.cos(angle), jnp.sin(angle)
    finish()
    full_in[tp] = jnp.sum(got_in[...], axis=0)
    finish = begin("tp", lambda t: full_in.at[tp], lambda t: full_in.at[t])
    for copy in loads[9:12]:
        copy.wait()
    finish()
    sums = jnp.concatenate([full_in[i] for i in range(n_tp)], axis=1)
    inv_in = lax.rsqrt(sums[:, q_rank + kv_rank + LANES :][:, :1] / d_model + EPS)
    lat_q = inv_in * sums[:, :q_rank]
    query_latent = (
        lat_q
        * lax.rsqrt(jnp.mean(lat_q * lat_q, axis=1, keepdims=True) + EPS)
        * wide(gain_q)
    ).astype(bf16)
    lat_kv = inv_in * sums[:, q_rank : q_rank + kv_rank]
    new_latent = (
        lat_kv
        * lax.rsqrt(jnp.mean(lat_kv * lat_kv, axis=1, keepdims=True) + EPS)
        * wide(gain_kv)
    ).astype(bf16)
    new_latent_ref[...] = new_latent
    new_latent = new_latent.astype(f32)
    new_rope = turn(
        inv_in * sums[:, q_rank + kv_rank : q_rank + kv_rank + LANES], cos, sin, half
    ).astype(bf16)
    new_rope_ref[...] = new_rope[:, :rope_size]
    new_rope = new_rope.astype(f32)[:, :rope_size]

    query_nope = dot_nt(query_latent, up_qn[...]).astype(bf16)
    times = heads * rope_size // LANES
    query_rope = turn(
        dot_nt(query_latent, up_qr[...]),
        jnp.concatenate([cos] * times, axis=1),
        jnp.concatenate([sin] * times, axis=1),
        half,
    ).astype(bf16).astype(f32)
    for h in range(heads):
        q_rows[h] = dot_nn(query_nope[:, h * nope : (h + 1) * nope], key_up[h]).astype(
            bf16
        ).astype(f32)
        r_rows[h] = query_rope[:, h * rope_size : (h + 1) * rope_size]

    for copy in loads[12:15]:
        copy.wait()
    first = me * rows
    at = first + lax.broadcasted_iota(jnp.int32, (heads, rows), 1)
    scores, selfs, lives = [], [], []
    for b in range(seqs):
        q_b = q_rows[:, b, :]
        r_b = r_rows[:, b, :]
        score = (
            dot_nt(q_b.astype(bf16), latent[b]) + dot_nn(r_b.astype(bf16), rope[b])
        ) * scale
        live = at < lengths[b]
        scores.append(jnp.where(live, score, -1e30))
        lives.append(live)
        own = (
            jnp.sum(q_b * new_latent[b : b + 1, :], axis=1, keepdims=True)
            + jnp.sum(r_b * new_rope[b : b + 1, :], axis=1, keepdims=True)
        ) * scale
        selfs.append(own)
    mine = me == 0
    for b in range(seqs):
        own = jnp.where(mine, selfs[b], -1e30)
        top = jnp.maximum(jnp.max(scores[b], axis=1, keepdims=True), own)
        weights = jnp.where(lives[b], jnp.exp(scores[b] - top), 0.0)
        own_weight = jnp.where(mine, jnp.exp(own - top), 0.0)
        total = jnp.sum(weights, axis=1, keepdims=True) + own_weight
        acc_rows[b, :, :kv_rank] = (
            dot_nn(weights.astype(bf16), latent[b])
            + own_weight.astype(bf16).astype(f32) * new_latent[b : b + 1, :]
        )
        acc_rows[b, :, kv_rank : kv_rank + LANES] = jnp.broadcast_to(top, (heads, LANES))
        acc_rows[b, :, kv_rank + LANES :] = jnp.broadcast_to(total, (heads, LANES))

    v_wide = own_heads * v_size
    for t in range(n_tp):
        pieces = []
        stat = jnp.zeros((seqs, LANES), f32)
        for i in range(own_heads):
            h = t * own_heads + i
            acc = acc_rows[:, h, :]
            exact = acc[:, :kv_rank]
            high = exact.astype(bf16)
            low = (exact - high.astype(f32)).astype(bf16)
            both = dot_nt(jnp.concatenate([high, low], axis=0), value_up[h])
            pieces.append(both[:seqs] + both[seqs:])
            stat = jnp.where(lane == i, acc[:, kv_rank : kv_rank + LANES], stat)
            stat = jnp.where(lane == own_heads + i, acc[:, kv_rank + LANES :], stat)
        part_att[t] = jnp.concatenate(pieces + [stat], axis=1)
    finish = begin("tp", lambda t: part_att.at[t], lambda t: got_att.at[t])
    got_att[tp] = part_att[tp]
    finish()

    stats = [got_att[t][:, v_wide:] for t in range(n_tp)]
    top = functools.reduce(jnp.maximum, stats)
    head_lane = lax.broadcasted_iota(jnp.int32, (seqs, v_wide), 1) // v_size
    joined = jnp.zeros((seqs, v_wide), f32)
    totals = jnp.zeros((seqs, LANES), f32)
    for t in range(n_tp):
        fade_t = jnp.exp(stats[t] - top)
        fade = jnp.zeros((seqs, v_wide), f32)
        for i in range(own_heads):
            fade = jnp.where(head_lane == i, fade_t[:, i : i + 1], fade)
        joined += got_att[t][:, :v_wide] * fade
        totals += stats[t] * pltpu.roll(fade_t, own_heads, 1)
    got_top[kv] = across(jnp.where(lane < own_heads, top, totals))[: got_top.shape[1], :]
    got_seq[kv] = joined
    finish_top = begin("kv", lambda k: got_top.at[kv], lambda k: got_top.at[k])
    finish = begin("kv", lambda k: got_seq.at[kv], lambda k: got_seq.at[k])
    loads[15].wait()
    finish_top()
    tops = [got_top[k][:own_heads, :] for k in range(n_kv)]
    top = functools.reduce(jnp.maximum, tops)
    fades = [jnp.exp(tops[k] - top) for k in range(n_kv)]
    total = sum(got_top[k][own_heads : 2 * own_heads, :] * fades[k] for k in range(n_kv))
    used = lax.broadcasted_iota(jnp.int32, total.shape, 1) < seqs
    share = 1.0 / jnp.where(used, total, 1.0)
    shares = across(jnp.concatenate([fade * share for fade in fades], axis=0))[:seqs, :]
    finish()
    head_sum = jnp.zeros((seqs, v_wide), f32)
    for k in range(n_kv):
        fade = jnp.zeros((seqs, v_wide), f32)
        for i in range(own_heads):
            at_lane = k * own_heads + i
            fade = jnp.where(head_lane == i, shares[:, at_lane : at_lane + 1], fade)
        head_sum += got_seq[k] * fade
    head_out = head_sum.astype(bf16)

    got_out[tp] = dot_nn(head_out, attn_out[...])
    finish = begin("tp", lambda t: got_out.at[tp], lambda t: got_out.at[t])
    loads[16].wait()
    finish()
    resid_mid = resid + jnp.sum(got_out[...], axis=0)
    got_stat[kv] = jnp.broadcast_to(
        jnp.sum(resid_mid * resid_mid, axis=1, keepdims=True), (seqs, LANES)
    )
    finish_stat = begin("kv", lambda k: got_stat.at[kv], lambda k: got_stat.at[k])
    scaled_mid = (resid_mid * wide(gain_mid)).astype(bf16)
    piece = ff_in.shape[1] // n_kv

    def hidden_of(k):
        columns = pl.ds(pl.multiple_of(k * piece, LANES), piece)
        return dot_nn(scaled_mid, ff_in[:, columns])

    def prepare(k):
        part_ff[k] = hidden_of(k)

    finish = begin("kv", lambda k: part_ff.at[k], lambda k: got_ff.at[k], n_kv // 2, prepare)
    got_ff[kv] = hidden_of(kv)
    finish_stat()
    inv_mid = lax.rsqrt(jnp.sum(got_stat[...], axis=0)[:, :1] / d_model + EPS)
    loads[17].wait()
    finish()
    full_ff[kv] = jnp.sum(got_ff[...], axis=0)
    finish = begin("kv", lambda k: full_ff.at[kv], lambda k: full_ff.at[k])
    out_parts = []

    def use(k):
        hidden = jnp.square(jnp.maximum(inv_mid * full_ff[k], 0.0)).astype(bf16)
        columns = pl.ds(pl.multiple_of(k * piece, LANES), piece)
        out_parts.append(dot_nn(hidden, ff_out[columns, :]))

    use(kv)
    finish(use)
    got_mix[tp] = sum(out_parts)
    finish = begin("tp", lambda t: got_mix.at[tp], lambda t: got_mix.at[t])
    finish()
    mixed_ref[...] = (resid_mid + jnp.sum(got_mix[...], axis=0)).astype(bf16)
    for copy in sent:
        copy.wait_send()


def hand_out(mixed, new_latent, new_rope, mixed_out, new_latent_out, new_rope_out):
    mixed_out[...] = mixed[...]
    new_latent_out[...] = new_latent[...]
    new_rope_out[...] = new_rope[...]


def per_device_kernel(
    n_kv, n_tp,
    tokens, lengths, latent_cache, rope_cache, gain_in, w_down_q, w_down_kv, w_rope_key, gain_q,
    w_up_qn, w_up_qr, gain_kv, w_key_up, w_value_up, w_attn_out, gain_mid, w_ff_in, w_ff_out,
):
    f32 = jnp.float32
    bf16 = jnp.bfloat16
    seqs, width = tokens.shape
    q_rank, heads, nope = w_up_qn.shape
    kv_rank, _, v_size = w_value_up.shape
    rope_size = w_rope_key.shape[1]
    hidden = w_ff_in.shape[1]
    v_wide = heads // n_tp * v_size
    top_rows = pl.cdiv(2 * (heads // n_tp), 8) * 8
    big = [
        tokens,
        gain_in,
        lengths,
        gain_q,
        gain_kv,
        gain_mid,
        latent_cache,
        rope_cache.transpose(0, 2, 1),
        w_down_q,
        w_down_kv,
        w_rope_key.T,
        w_up_qn.transpose(1, 2, 0).reshape(heads * nope, q_rank),
        w_up_qr.transpose(1, 2, 0).reshape(heads * rope_size, q_rank),
        w_key_up.transpose(1, 2, 0),
        w_value_up.transpose(1, 2, 0),
        w_attn_out.reshape(-1, width),
        w_ff_in,
        w_ff_out,
    ]
    block = (q_rank + kv_rank + 2 * LANES) // n_tp
    messages = 6 * (n_kv - 1) + 4 * (n_tp - 1)
    vmem = pltpu.VMEM
    whole = pl.BlockSpec(memory_space=pltpu.VMEM)
    results = pl.pallas_call(
        functools.partial(layer_kernel, n_kv, n_tp),
        out_shape=(
            pltpu.VMEM((seqs, width), bf16),
            pltpu.VMEM((seqs, kv_rank), bf16),
            pltpu.VMEM((seqs, rope_size), bf16),
        ),
        in_specs=[pl.BlockSpec(memory_space=pl.ANY)] * len(big),
        out_specs=(whole, whole, whole),
        scratch_shapes=[
            pltpu.SMEM(a.shape, a.dtype) if a is lengths else vmem(a.shape, a.dtype) for a in big
        ]
        + [
            vmem((n_tp, seqs, block), f32),
            vmem((n_kv, seqs, block), f32),
            vmem((n_tp, seqs, block), f32),
            vmem((heads, seqs, kv_rank), f32),
            vmem((heads, seqs, rope_size), f32),
            vmem((seqs, heads, kv_rank + 2 * LANES), f32),
            vmem((n_tp, seqs, v_wide + LANES), f32),
            vmem((n_tp, seqs, v_wide + LANES), f32),
            vmem((n_kv, top_rows, LANES), f32),
            vmem((n_kv, seqs, v_wide), f32),
            vmem((n_tp, seqs, width), f32),
            vmem((n_kv, seqs, LANES), f32),
            vmem((n_kv, seqs, hidden // n_kv), f32),
            vmem((n_kv, seqs, hidden // n_kv), f32),
            vmem((n_kv, seqs, hidden // n_kv), f32),
            vmem((n_tp, seqs, width), f32),
            pltpu.SemaphoreType.DMA((len(big),)),
            pltpu.SemaphoreType.DMA((messages,)),
            pltpu.SemaphoreType.DMA((messages,)),
        ],
        compiler_params=pltpu.CompilerParams(collective_id=0, has_side_effects=True),
        name="layer",
    )(*big)
    return pl.pallas_call(
        hand_out,
        out_shape=tuple(jax.ShapeDtypeStruct(a.shape, a.dtype) for a in results),
        in_specs=[whole] * 3,
        out_specs=(whole,) * 3,
        name="hand_out",
    )(*(pltpu.with_memory_space_constraint(a, pltpu.VMEM) for a in results))


def kernel_fits(n_kv, n_tp, seqs, width, q_rank, kv_rank, rope_size, heads, v_size, hidden):
    return (
        heads % n_tp == 0
        and seqs <= LANES
        and n_kv * (heads // n_tp) <= LANES
        and width % LANES == 0
        and q_rank % LANES == 0
        and kv_rank % LANES == 0
        and LANES % rope_size == 0
        and (heads * rope_size) % LANES == 0
        and (q_rank + kv_rank + 2 * LANES) % (n_tp * LANES) == 0
        and (heads // n_tp * v_size) % LANES == 0
        and hidden % (n_kv * LANES) == 0
    )


def per_device_any(n_kv, n_tp, *args):
    tokens, w_down_q, w_down_kv, w_rope_key = args[0], args[5], args[6], args[7]
    w_value_up, w_ff_in = args[13], args[16]
    if kernel_fits(
        n_kv, n_tp, *tokens.shape, w_down_q.shape[1], w_down_kv.shape[1], w_rope_key.shape[1],
        *w_value_up.shape[1:], w_ff_in.shape[1],
    ):
        return per_device_kernel(n_kv, n_tp, *args)
    return per_device(*args)


def solution(mesh):
    return jax.shard_map(
        functools.partial(per_device_any, mesh.shape["kv"], mesh.shape["tp"]),
        mesh=mesh,
        in_specs=(
            P(None, "kv"),
            P(),
            P(None, ("kv", "tp"), None),
            P(None, ("kv", "tp"), None),
            P("kv"),
            P("kv", None),
            P("kv", None),
            P("kv", None),
            P(),
            P(),
            P(),
            P(),
            P(),
            P(),
            P("tp", None, "kv"),
            P("kv"),
            P("kv", "tp"),
            P("tp", "kv"),
        ),
        out_specs=(P(None, "kv"), P(), P()),
        check_vma=False,
    )
```
